32 devices in a mesh: ep: 8 (over z, core), tp: 4 (over y, x).
Axes of the slice: x: 2, y: 2, z: 4, core: 2. Of those that a mesh axis runs over, the one named last changes fastest.
Arguments:
- queries: bfloat16 [1024, 1536], P('ep', 'tp'), may hold values from -64 to 64
- kv_latent: bfloat16 [1024, 512], P('ep'), may hold values from -60 to 60
- rope_key: bfloat16 [1024, 32], P('ep'), may hold values from -64 to 64
- latent_gain: float32 [512], replicated, may hold values from 0.1 to 1.9
- key_up: bfloat16 [512, 1024], P(None, 'tp'), may hold values from -0.25 to 0.25
- value_up: bfloat16 [512, 1024], P(None, 'tp'), may hold values from -40 to 40
- query_gain: float32 [96], replicated, may hold values from 0.3 to 4
- key_gain: float32 [96], replicated, may hold values from 0.3 to 4
- out_gain: float32 [1024], replicated, may hold values from 0.1 to 1.9
- out_proj: bfloat16 [1024, 4096], P(None, 'tp'), may hold values from -0.1875 to 0.1875
- moe_input: bfloat16 [1024, 4096], P('ep'), may hold values from -60 to 60
- moe_gain: float32 [4096], replicated, may hold values from 0.1 to 1.9
- expert_ids: int32 [1024, 2], P('ep'), may hold values from 0 to 31, as said below
- route_weights: float32 [1024, 2], P('ep'), may hold values from 0.2 to 1
- w_gate: bfloat16 [32, 4096, 2048], P('ep', None, 'tp'), may hold values from -0.09375 to 0.09375
- w_up: bfloat16 [32, 4096, 2048], P('ep', None, 'tp'), may hold values from -0.09375 to 0.09375
- w_down: bfloat16 [32, 2048, 4096], P('ep', 'tp'), may hold values from -0.125 to 0.125
Outputs:
- mixed: bfloat16 [1024, 4096], P('ep', 'tp')
- expert_out: bfloat16 [1024, 4096], P('ep', 'tp')
The draws below stay inside these ranges and needn't reach their ends.
Inputs may be any that keep to these rules, and one draw needn't show every extreme that they name: `expert_ids`: both experts of a row lie in one group (g * 8 to g * 8 + 7) and differ. In each aligned block of 128 rows no expert is named more than 12 times, and some expert is named exactly 12 times.
All inputs are finite; a program needn't handle non-finite values.
Results may differ from the reference program's by a relative error of at most 0.015.
The reference program's roundings to bfloat16 on the way count: a program that leaves them out, or rounds other values in their place, can miss the bound.
Values may be sent and summed in bfloat16 or wider, within the bound.
A program may use at most 128 MiB of HBM per device.

```python
import jax
import jax.numpy as jnp
from jax import lax

D = 4096
HEADS = 16
NOPE = 64
ROPE = 32
VDIM = 64
KV_RANK = 512
PER_GROUP = 8
D_EXP = 2048
TOP = 2
TOK_DEV = 128
QKD = 96
EXPERTS = 32
TOKENS = 1024
CAP = 12
N_EP = 8
N_TP = 4


def draw_rope_key(key, part):
    drawn = jnp.clip(jax.random.normal(jax.random.fold_in(key, 21), (TOKENS, ROPE), jnp.float32), -6.0, 6.0)
    return drawn.astype(jnp.bfloat16)


def draw_queries(key, part):
    drawn = jnp.clip(jax.random.normal(jax.random.fold_in(key, 31), (TOKENS, HEADS, QKD), jnp.float32), -6.0, 6.0)
    return drawn.reshape(TOKENS, HEADS * QKD).astype(jnp.bfloat16)


def draw_query_gain(key, part):
    drawn = jax.random.uniform(jax.random.fold_in(key, 41), (QKD,), jnp.float32, 0.3, 1.7)
    return drawn


def draw_key_gain(key, part):
    drawn = jax.random.uniform(jax.random.fold_in(key, 51), (QKD,), jnp.float32, 0.3, 1.7)
    return drawn


def scaled_rows(key, salt, row_count, col_count):
    drawn = jnp.clip(jax.random.normal(jax.random.fold_in(key, salt), (row_count, col_count), jnp.float32), -6.0, 6.0)
    return drawn


def draw_kv_latent(key, part):
    return scaled_rows(key, 61, TOKENS, KV_RANK).astype(jnp.bfloat16)


def draw_moe_input(key, part):
    return scaled_rows(key, 71, TOKENS, D).astype(jnp.bfloat16)


def draw_value_up(key, part):
    drawn = jax.random.normal(jax.random.fold_in(key, 81), (KV_RANK, HEADS * VDIM), jnp.float32) * KV_RANK ** (-0.5)
    head_pos = (jnp.arange(HEADS * VDIM) // VDIM).astype(jnp.float32) / (HEADS - 1)
    scale = 3.0 ** head_pos
    return jnp.clip(drawn * scale[None, :], -40.0, 40.0).astype(jnp.bfloat16)


def draw_expert_ids(key, part):
    block_keys = jax.random.split(jax.random.fold_in(key, 91), TOKENS // TOK_DEV)

    def one_block(block_key):
        parts_key = jax.random.split(block_key, 6)
        biggest = jax.random.randint(parts_key[0], (), 0, 4)
        low_count = TOK_DEV // 8
        high_count = TOK_DEV // 4
        count_a = jax.random.randint(parts_key[1], (), low_count, high_count + 1)
        count_b = jax.random.randint(parts_key[2], (), low_count, high_count + 1)
        count_c = 5 * TOK_DEV // 8 - count_a - count_b
        others = (biggest + 1 + jnp.arange(3)) % 4
        counts = jnp.zeros((4,), jnp.int32).at[biggest].set(3 * TOK_DEV // 8)
        counts = counts.at[others].set(jnp.stack([count_a, count_b, count_c]).astype(jnp.int32))
        ends = jnp.cumsum(counts)
        ranks = jnp.arange(TOK_DEV)
        group_of = jnp.sum((ranks[:, None] >= ends[None, :]).astype(jnp.int32), axis=1)
        within = ranks - (ends - counts)[group_of]
        shifts = jax.random.randint(parts_key[3], (4,), 0, PER_GROUP)
        steps_apart = jax.random.randint(parts_key[4], (4,), 1, PER_GROUP)
        first_pick = (shifts[group_of] + within) % PER_GROUP
        second_pick = (shifts[group_of] + within + steps_apart[group_of]) % PER_GROUP
        chosen = jnp.stack([first_pick, second_pick], axis=1) + group_of[:, None] * PER_GROUP
        order = jax.random.permutation(parts_key[5], TOK_DEV)
        return chosen[order]
    return jax.vmap(one_block)(block_keys).reshape(TOKENS, 2).astype(jnp.int32)


def block_levels(own_key, shape, cuts, low, largest):
    factor_of, own = 1.0, jax.random.fold_in(own_key, 6)
    for dim, blocks in cuts:
        draws = jnp.exp(jax.random.uniform(jax.random.fold_in(own, dim), (blocks,), jnp.float32, low / len(cuts), largest / len(cuts)))
        factor_of = factor_of * jnp.repeat(draws, shape[dim] // blocks).reshape([-1 if axis == dim else 1 for axis in range(len(shape))])
    return factor_of


def noise(key, dims, deviation, most, cuts=(), kind=jnp.bfloat16):
    entries = jax.random.normal(key, dims, jnp.float32) * deviation
    if len(cuts) > 0:
        entries = block_levels(key, dims, cuts, -0.22, 0.18) * entries
    return jnp.clip(entries, min=-most, max=most).astype(kind)


def setup_inputs(seed: int = 0) -> dict:
    seeds = jax.random.split(jax.random.key(seed), 18)
    return {
        "queries": draw_queries(jax.random.fold_in(seeds[17], 71), 0),
        "kv_latent": draw_kv_latent(jax.random.fold_in(seeds[17], 71), 0),
        "rope_key": draw_rope_key(jax.random.fold_in(seeds[17], 71), 0),
        "latent_gain": jnp.clip(1.0 + 0.18 * jax.random.normal(seeds[3], (KV_RANK,), jnp.float32), 0.1, 1.9),
        "key_up": noise(seeds[4], (KV_RANK, HEADS * NOPE), KV_RANK ** -0.5, 0.25, ((1, 4),)),
        "value_up": draw_value_up(jax.random.fold_in(seeds[17], 71), 0),
        "query_gain": draw_query_gain(jax.random.fold_in(seeds[17], 71), 0),
        "key_gain": draw_key_gain(jax.random.fold_in(seeds[17], 71), 0),
        "out_gain": jnp.clip(1.0 + 0.18 * jax.random.normal(seeds[8], (HEADS * VDIM,), jnp.float32), 0.1, 1.9),
        "out_proj": noise(seeds[9], (HEADS * VDIM, D), (HEADS * VDIM) ** -0.5, 0.1875, ((1, 4),)),
        "moe_input": draw_moe_input(jax.random.fold_in(seeds[17], 71), 0),
        "moe_gain": jnp.clip(1.0 + 0.18 * jax.random.normal(seeds[11], (D,), jnp.float32), 0.1, 1.9),
        "expert_ids": draw_expert_ids(jax.random.fold_in(seeds[17], 71), 0),
        "route_weights": jnp.clip(0.2 + 0.8 * jax.random.uniform(seeds[13], (TOKENS, TOP), jnp.float32) ** block_levels(seeds[13], (TOKENS, TOP), ((0, 8),), -0.2, 0.2), 0.2, 1.0),
        "w_gate": noise(seeds[14], (EXPERTS, D, D_EXP), D ** -0.5, 0.09375, ((0, 8), (2, 4))),
        "w_up": noise(seeds[15], (EXPERTS, D, D_EXP), D ** -0.5, 0.09375, ((0, 8), (2, 4))),
        "w_down": noise(seeds[16], (EXPERTS, D_EXP, D), D_EXP ** -0.5, 0.125, ((0, 8), (1, 4))),
    }


EPS = 1e-06
THETA = 10000.0

def rotate_half(values_in, positions):
    half_width = ROPE // 2
    inverse = THETA ** (-jnp.arange(half_width, dtype=jnp.float32) / half_width)
    angles = positions.astype(jnp.float32)[:, None] * inverse
    cosine = jnp.cos(angles)[:, None, :]
    sine = jnp.sin(angles)[:, None, :]
    first_half = values_in[..., :half_width]
    second_half = values_in[..., half_width:]
    return jnp.concatenate([first_half * cosine - second_half * sine, second_half * cosine + first_half * sine], axis=-1)

def head_norm(values_in, gain_vec):
    return values_in * lax.rsqrt(lax.optimization_barrier(jnp.mean(values_in * values_in, axis=-1, keepdims=True)) + EPS) * gain_vec

def make_queries(queries, query_gain, positions):
    row_count = queries.shape[0]
    head_count = queries.shape[1] // QKD
    normed = head_norm(queries.astype(jnp.float32).reshape(row_count, head_count, QKD), query_gain)
    turned = jnp.concatenate([normed[..., :NOPE], rotate_half(normed[..., NOPE:], positions)], axis=-1)
    return turned.astype(jnp.bfloat16)

def make_keys(latent, rope_part, latent_gain, key_up, value_up, key_gain, positions):
    row_count = latent.shape[0]
    head_count = key_up.shape[1] // NOPE
    latent_f = latent.astype(jnp.float32)
    latent_n = (latent_f * lax.rsqrt(lax.optimization_barrier(jnp.mean(latent_f * latent_f, axis=-1, keepdims=True)) + EPS) * latent_gain).astype(jnp.bfloat16)
    key_nope = jnp.dot(latent_n, key_up, preferred_element_type=jnp.float32).astype(jnp.bfloat16)
    key_nope = lax.optimization_barrier(key_nope)
    value_rows = jnp.dot(latent_n, value_up, preferred_element_type=jnp.float32).astype(jnp.bfloat16)
    shared = jnp.broadcast_to(rope_part.astype(jnp.float32)[:, None, :], (row_count, head_count, ROPE))
    key_full = jnp.concatenate([key_nope.astype(jnp.float32).reshape(row_count, head_count, NOPE), shared], axis=-1)
    normed = head_norm(key_full, key_gain)
    turned = jnp.concatenate([normed[..., :NOPE], rotate_half(normed[..., NOPE:], positions)], axis=-1)
    return (turned.astype(jnp.bfloat16), value_rows.reshape(row_count, head_count, VDIM))

def attention(query_rot, key_rot, value_rows):
    block_rows = 512
    block_count = TOKENS // block_rows
    key_pos = jnp.arange(TOKENS)
    keys_f = key_rot.astype(jnp.float32)
    values_f = value_rows.astype(jnp.float32)
    head_count = query_rot.shape[1]

    def one_block(index):
        first = index * block_rows
        query_blk = lax.dynamic_slice_in_dim(query_rot, first, block_rows, 0).astype(jnp.float32)
        scores = jnp.einsum('qhd,khd->hqk', query_blk, keys_f) * QKD ** (-0.5)
        query_pos = first + jnp.arange(block_rows)
        visible = key_pos[None, :] <= query_pos[:, None]
        scores = jnp.where(visible[None], scores, -1e+30)
        top_score = lax.optimization_barrier(jnp.max(scores, axis=-1, keepdims=True))
        expo = jnp.exp(scores - top_score)
        probs = lax.optimization_barrier(expo.astype(jnp.bfloat16))
        totals = lax.optimization_barrier(jnp.sum(expo, axis=-1))
        weighted = jnp.einsum('hqk,khd->hqd', probs.astype(jnp.float32), values_f) / totals[..., None]
        return weighted.astype(jnp.bfloat16)
    outcome = lax.map(one_block, jnp.arange(block_count))
    return outcome.transpose(0, 2, 1, 3).reshape(TOKENS, head_count * VDIM)

def reference(queries, kv_latent, rope_key, latent_gain, key_up, value_up, query_gain, key_gain, out_gain, out_proj, moe_input, moe_gain, expert_ids, route_weights, w_gate, w_up, w_down):
    positions = jnp.arange(TOKENS, dtype=jnp.int32)
    query_rot = make_queries(queries, query_gain, positions)
    key_rot, value_rows = make_keys(kv_latent, rope_key, latent_gain, key_up, value_up, key_gain, positions)
    attn = attention(query_rot, key_rot, value_rows)
    attn_f = attn.astype(jnp.float32)
    inverse_rms = lax.rsqrt(lax.optimization_barrier(jnp.mean(attn_f * attn_f, axis=-1)) + EPS)
    attn_n = (attn_f * out_gain).astype(jnp.bfloat16)
    mixed = (jnp.dot(attn_n, out_proj, preferred_element_type=jnp.float32) * inverse_rms[:, None]).astype(jnp.bfloat16)
    stream_f = moe_input.astype(jnp.float32)
    normed = (stream_f * lax.rsqrt(lax.optimization_barrier(jnp.mean(stream_f * stream_f, axis=-1, keepdims=True)) + EPS) * moe_gain).astype(jnp.bfloat16)
    flat_ids = expert_ids.reshape(-1).astype(jnp.int32)
    pick_count = TOKENS * TOP
    onehot = (flat_ids[:, None] == jnp.arange(EXPERTS, dtype=jnp.int32)[None, :]).astype(jnp.int32)
    per_block = onehot.reshape(N_EP, TOK_DEV * TOP, EXPERTS)
    earlier = (jnp.cumsum(per_block, axis=1) - per_block).astype(jnp.int32)
    slot_rank = lax.optimization_barrier(jnp.sum(earlier * per_block, axis=-1)).reshape(-1).astype(jnp.int32)
    block_index = (jnp.arange(pick_count, dtype=jnp.int32) // (TOK_DEV * TOP)).astype(jnp.int32)
    slot_count = N_EP * CAP
    slot_index = (flat_ids * slot_count + block_index * CAP + slot_rank).astype(jnp.int32)
    token_index = (jnp.arange(pick_count, dtype=jnp.int32) // TOP).astype(jnp.int32)
    slot_token = jnp.zeros((EXPERTS * slot_count,), jnp.int32).at[slot_index].set(token_index)
    expert_rows = normed[slot_token].reshape(EXPERTS, slot_count, D)
    shard_width = D_EXP // N_TP

    def one_expert(operands):
        rows_in, gate_w, up_w, down_w = operands
        gate = jnp.dot(rows_in, gate_w, preferred_element_type=jnp.float32)
        upper = jnp.dot(rows_in, up_w, preferred_element_type=jnp.float32)
        act = (jax.nn.silu(gate) * upper).astype(jnp.bfloat16)
        partials = jnp.einsum('sjf,jfd->jsd', act.reshape(slot_count, N_TP, shard_width).astype(jnp.float32), down_w.reshape(N_TP, shard_width, D).astype(jnp.float32))
        partials = lax.optimization_barrier(partials.astype(jnp.bfloat16))
        return lax.optimization_barrier(jnp.sum(partials.astype(jnp.float32), axis=0)).astype(jnp.bfloat16)
    expert_y = lax.map(one_expert, (expert_rows, w_gate, w_up, w_down)).reshape(EXPERTS * slot_count, D)
    picked = expert_y[slot_index].reshape(TOKENS, TOP, D).astype(jnp.float32)
    expert_out = lax.optimization_barrier(jnp.sum(picked * route_weights[..., None], axis=1)).astype(jnp.bfloat16)
    return (mixed, expert_out)
```

```python
import functools

import jax
import jax.numpy as jnp
import numpy as np
from jax import lax
from jax.experimental import pallas as pl
from jax.experimental.pallas import tpu as pltpu
from jax.sharding import PartitionSpec as P

NOPE = 64
ROPE = 32
VDIM = 64
QKD = 96
CAP = 12


EPS = 1e-06
THETA = 10000.0


def rotate_half(values_in, positions):
    half_width = ROPE // 2
    inverse = THETA ** (-jnp.arange(half_width, dtype=jnp.float32) / half_width)
    angles = positions.astype(jnp.float32)[:, None] * inverse
    cosine = jnp.cos(angles)[:, None, :]
    sine = jnp.sin(angles)[:, None, :]
    first_half = values_in[..., :half_width]
    second_half = values_in[..., half_width:]
    return jnp.concatenate(
        [first_half * cosine - second_half * sine, second_half * cosine + first_half * sine],
        axis=-1,
    )


def head_norm(values_in, gain_vec):
    return (
        values_in
        * lax.rsqrt(jnp.mean(values_in * values_in, axis=-1, keepdims=True) + EPS)
        * gain_vec
    )


def make_queries(queries, query_gain, positions):
    row_count = queries.shape[0]
    head_count = queries.shape[1] // QKD
    normed = head_norm(queries.astype(jnp.float32).reshape(row_count, head_count, QKD), query_gain)
    turned = jnp.concatenate(
        [normed[..., :NOPE], rotate_half(normed[..., NOPE:], positions)], axis=-1
    )
    return turned.astype(jnp.bfloat16)


def make_keys(latent, rope_part, latent_gain, key_up, value_up, key_gain, positions):
    row_count = latent.shape[0]
    head_count = key_up.shape[1] // NOPE
    latent_f = latent.astype(jnp.float32)
    latent_n = (
        latent_f
        * lax.rsqrt(jnp.mean(latent_f * latent_f, axis=-1, keepdims=True) + EPS)
        * latent_gain
    ).astype(jnp.bfloat16)
    key_nope = jnp.dot(latent_n, key_up, preferred_element_type=jnp.float32).astype(jnp.bfloat16)
    key_nope = lax.optimization_barrier(key_nope)
    value_rows = jnp.dot(latent_n, value_up, preferred_element_type=jnp.float32).astype(
        jnp.bfloat16
    )
    shared = jnp.broadcast_to(
        rope_part.astype(jnp.float32)[:, None, :], (row_count, head_count, ROPE)
    )
    key_full = jnp.concatenate(
        [key_nope.astype(jnp.float32).reshape(row_count, head_count, NOPE), shared], axis=-1
    )
    normed = head_norm(key_full, key_gain)
    turned = jnp.concatenate(
        [normed[..., :NOPE], rotate_half(normed[..., NOPE:], positions)], axis=-1
    )
    return (turned.astype(jnp.bfloat16), value_rows.reshape(row_count, head_count, VDIM))


def shards(
    queries,
    kv_latent,
    rope_key,
    latent_gain,
    key_up,
    value_up,
    query_gain,
    key_gain,
    out_gain,
    out_proj,
    moe_input,
    moe_gain,
    expert_ids,
    route_weights,
    w_gate,
    w_up,
    w_down,
):
    tok_rows = queries.shape[0]
    head_count = key_up.shape[1] // NOPE
    query_pos = lax.axis_index("ep") * tok_rows + jnp.arange(tok_rows, dtype=jnp.int32)
    query_rot = make_queries(queries, query_gain, query_pos)
    inv_scale = QKD ** (-0.5)
    blocks_in = (
        lax.all_gather(kv_latent, "ep", axis=0, tiled=True),
        lax.all_gather(rope_key, "ep", axis=0, tiled=True),
    )
    key_pos = jnp.arange(blocks_in[0].shape[0], dtype=jnp.int32)
    key_rot, value_rows = make_keys(
        blocks_in[0], blocks_in[1], latent_gain, key_up, value_up, key_gain, key_pos
    )
    top_prev = jnp.full((head_count, tok_rows), -1e30, jnp.float32)
    key_pos = jnp.arange(key_rot.shape[0], dtype=jnp.int32)
    scores = (
        jnp.einsum("qhd,khd->hqk", query_rot, key_rot, preferred_element_type=jnp.float32)
        * inv_scale
    )
    visible = key_pos[None, :] <= query_pos[:, None]
    scores = jnp.where(visible[None], scores, -1e30)
    top_new = jnp.maximum(top_prev, jnp.max(scores, axis=-1))
    expo = jnp.exp(scores - top_new[..., None])
    total_new = jnp.sum(expo, axis=-1)
    accum_new = jnp.einsum(
        "hqk,khd->hqd", expo.astype(jnp.bfloat16), value_rows, preferred_element_type=jnp.float32
    )
    attn = (accum_new / total_new[..., None]).astype(jnp.bfloat16)
    attn = attn.transpose(1, 0, 2).reshape(tok_rows, head_count * VDIM)
    block_f = lax.all_gather(attn, "tp", axis=1, tiled=True).astype(jnp.float32)
    scaled = (block_f * out_gain[None, :]).astype(jnp.bfloat16)
    product = jnp.dot(scaled, out_proj, preferred_element_type=jnp.float32)
    product, squares = (product, jnp.sum(block_f * block_f, axis=-1))
    mixed = (product * lax.rsqrt(squares / out_gain.shape[0] + EPS)[:, None]).astype(jnp.bfloat16)
    row_count = moe_input.shape[0]
    top_count = expert_ids.shape[1]
    local_experts = w_gate.shape[0]
    ep_count = lax.axis_size("ep")
    expert_count = local_experts * ep_count
    stream_f = moe_input.astype(jnp.float32)
    normed = (
        stream_f * lax.rsqrt(jnp.mean(stream_f * stream_f, axis=-1, keepdims=True) + EPS) * moe_gain
    ).astype(jnp.bfloat16)
    flat_ids = expert_ids.reshape(-1)
    onehot = (flat_ids[:, None] == jnp.arange(expert_count, dtype=jnp.int32)[None, :]).astype(
        jnp.int32
    )
    slot_rank = jnp.sum((jnp.cumsum(onehot, axis=0) - onehot) * onehot, axis=1)
    slot_index = flat_ids * CAP + slot_rank
    token_index = jnp.arange(row_count * top_count, dtype=jnp.int32) // top_count
    slot_token = jnp.zeros((expert_count * CAP,), jnp.int32).at[slot_index].set(token_index)
    slot_used = jnp.zeros((expert_count * CAP,), jnp.bool_).at[slot_index].set(True)
    outgoing = jnp.where(slot_used[:, None], normed[slot_token], jnp.zeros((), jnp.bfloat16))
    outgoing = outgoing.reshape(ep_count, local_experts, CAP, normed.shape[1])
    piece_width = normed.shape[1] // lax.axis_size("tp")
    my_columns = lax.dynamic_slice_in_dim(
        outgoing, lax.axis_index("tp") * piece_width, piece_width, 3
    )
    arrived_part = lax.all_to_all(my_columns, "ep", split_axis=0, concat_axis=0, tiled=True)
    piece = lax.all_gather(arrived_part, "tp", axis=3, tiled=True)
    gate_acc = jnp.einsum("secd,edf->secf", piece, w_gate, preferred_element_type=jnp.float32)
    upper_acc = jnp.einsum("secd,edf->secf", piece, w_up, preferred_element_type=jnp.float32)
    hidden = (jax.nn.silu(gate_acc) * upper_acc).astype(jnp.bfloat16)
    out_cols = w_down.shape[2] // lax.axis_size("tp")
    term = jnp.einsum("secf,efd->dsec", hidden, w_down, preferred_element_type=jnp.float32)
    summed = lax.psum_scatter(
        term.reshape(lax.axis_size("tp") * out_cols, -1).astype(jnp.bfloat16),
        "tp",
        scatter_dimension=0,
        tiled=True,
    )
    expert_y = summed.T.reshape(ep_count, local_experts * CAP, out_cols)
    returned_rows = lax.all_to_all(expert_y, "ep", split_axis=0, concat_axis=0, tiled=True).reshape(
        expert_count * CAP, out_cols
    )
    picked = returned_rows[slot_index].reshape(row_count, top_count, out_cols).astype(jnp.float32)
    expert_out = jnp.sum(picked * route_weights[..., None], axis=1).astype(jnp.bfloat16)
    return (mixed, expert_out)


MESH = pl.DeviceIdType.MESH
GROUP = 8
PAD = 128


def group_cap():
    return GROUP * CAP // 2


def rdma(src, dst, send_sem, recv_sem, device):
    copy = pltpu.make_async_remote_copy(
        src_ref=src,
        dst_ref=dst,
        send_sem=send_sem,
        recv_sem=recv_sem,
        device_id=device,
        device_id_type=MESH,
    )
    copy.start()
    return copy


def arrived(dst, sem, device):
    pltpu.make_async_remote_copy(
        src_ref=dst,
        dst_ref=dst,
        send_sem=sem,
        recv_sem=sem,
        device_id=device,
        device_id_type=MESH,
    ).wait_recv()


def places(planes):
    ep = lax.axis_index("ep")
    tp = lax.axis_index("tp")
    plane = ep // 2
    core = ep % 2

    def along(offset):
        return (lax.rem(plane + offset + planes, planes) * 2 + core, tp)

    partner = (plane * 2 + 1 - core, tp)
    near_x = (ep, tp ^ 1)
    near_y = (ep, tp ^ 2)
    corner = (ep, tp ^ 3)
    return tp, along, partner, near_x, near_y, corner


def greet(peers):
    barrier = pltpu.get_barrier_semaphore()
    for peer in peers:
        pl.semaphore_signal(barrier, inc=1, device_id=peer, device_id_type=MESH)
    pl.semaphore_wait(barrier, len(peers))


def rope_table(total):
    half = ROPE // 2
    inverse = np.float32(THETA) ** (-np.arange(half, dtype=np.float32) / np.float32(half))
    angles = np.arange(total, dtype=np.float32)[None, :] * inverse[:, None]
    return np.concatenate([np.cos(angles), np.sin(angles)], axis=0).astype(np.float32)


def turn(first_half, second_half, cosine, sine):
    return (
        first_half * cosine - second_half * sine,
        second_half * cosine + first_half * sine,
    )


def to_column(row):
    size = row.shape[1]
    rows = lax.broadcasted_iota(jnp.int32, (size, size), 0)
    cols = lax.broadcasted_iota(jnp.int32, (size, size), 1)
    return jnp.sum(jnp.where(rows == cols, row, 0.0), axis=1, keepdims=True)


def layer_kernel(
    planes,
    queries_in,
    latent_in,
    rope_in,
    latent_gain_in,
    key_up_in,
    value_up_in,
    query_gain_in,
    key_gain_in,
    out_gain_in,
    out_proj_in,
    stream_in,
    moe_gain_in,
    ids_in,
    weights_in,
    gate_ref,
    up_ref,
    down_ref,
    table_in,
    mixed_ref,
    expert_ref,
    queries_v,
    latent_v,
    latent_gain_v,
    key_up_v,
    value_up_v,
    query_gain_v,
    key_gain_v,
    out_gain_v,
    out_proj_v,
    stream_v,
    moe_gain_v,
    ids_v,
    weights_v,
    table_v,
    wbuf,
    latents,
    ropes,
    outgoing,
    metas_out,
    rows_ref,
    metas,
    turned_q,
    turned_k,
    values_v,
    heads,
    select_t,
    place_v,
    place_t,
    slot_w,
    taken,
    gate_acc,
    up_acc,
    hidden_v,
    given,
    part,
    other,
    bx1,
    by1,
    bx2,
    by2,
    done,
    back,
    loc,
    ws,
    zs,
    zr,
    xs,
    xr,
    ks,
    kr,
    ps,
    pr,
    hs,
    hr,
    cs,
    cr,
    rs,
    rr,
    bs,
    br,
):
    f32, bf = jnp.float32, jnp.bfloat16
    ep = lax.axis_index("ep")
    plane, core = ep // 2, ep % 2
    tp, along, partner, near_x, near_y, corner = places(planes)
    peers = [along(d) for d in range(1, planes)] + [partner, near_x, near_y, corner]
    barrier = pltpu.get_barrier_semaphore()
    for peer in peers:
        pl.semaphore_signal(barrier, inc=1, device_id=peer, device_id_type=MESH)

    blocks = 2 * planes
    tokens, model = stream_in.shape
    cap, width = outgoing.shape[1], outgoing.shape[2]
    experts, hidden = gate_ref.shape[0], gate_ref.shape[2]
    row_total, slots = blocks * cap, blocks * CAP
    slot_total = experts * slots
    quarter_rows = tokens // 4
    half_r, half_w = quarter_rows // 2, width // 2
    low, high = pl.ds(0, half_w), pl.ds(half_w, half_w)
    halves = (low, high)
    head_count = key_up_in.shape[1] // NOPE
    order = list(range(1, planes))
    turned = (((0,), (0,)), ((), ()))
    across = (((1,), (1,)), ((), ()))

    loads = {}

    def load(name, source, target):
        copy = pltpu.make_async_copy(source, target, loc.at[len(loads)])
        copy.start()
        loads[name] = copy

    load("latent", latent_in, latent_v)
    load("latent_gain", latent_gain_in, latent_gain_v)
    load("rope", rope_in, ropes.at[0, 0])
    load("stream", stream_in, stream_v)
    load("moe_gain", moe_gain_in, moe_gain_v)
    load("ids", ids_in, ids_v)
    load("weights", weights_in, weights_v)

    sent = []

    def send(src, dst, send_sem, recv_sem, device):
        sent.append(rdma(src, dst, send_sem, recv_sem, device))

    def quarter(which):
        return pl.ds(pl.multiple_of(which * quarter_rows, quarter_rows), quarter_rows)

    loads["latent"].wait()
    loads["latent_gain"].wait()
    latent_f = latent_v[...].astype(f32)
    latents[0, 0] = (
        latent_f
        * lax.rsqrt(jnp.mean(latent_f * latent_f, axis=-1, keepdims=True) + EPS)
        * latent_gain_v[...]
    ).astype(bf)
    loads["rope"].wait()
    pl.semaphore_wait(barrier, len(peers))
    own_part = latents.at[0, 0, quarter(tp)]
    for d in order:
        send(own_part, latents.at[0, d, quarter(tp)], zs.at[0, d], zr.at[0, d], along(d))
        send(ropes.at[0, 0], ropes.at[0, d], zs.at[1, d], zr.at[1, d], along(d))
    send(latents.at[0, 0], latents.at[1, 0], ks.at[0, 0], kr.at[0, 0], partner)
    send(ropes.at[0, 0], ropes.at[1, 0], ks.at[1, 0], kr.at[1, 0], partner)

    loads["stream"].wait()
    loads["moe_gain"].wait()
    loads["ids"].wait()
    loads["weights"].wait()
    load("queries", queries_in, queries_v)
    load("query_gain", query_gain_in, query_gain_v)
    load("key_gain", key_gain_in, key_gain_v)
    load("table", table_in, table_v)
    load("key_up", key_up_in, key_up_v)
    load("value_up", value_up_in, value_up_v)
    gate_in, up_in, down_in = [], [], {}
    for s in range(4):
        depth = pl.ds(pl.multiple_of((tp ^ s) * width, width), width)
        gate_in.append(
            pltpu.make_async_copy(gate_ref.at[:, depth, :], wbuf.at[s], ws.at[0, s])
        )
        up_in.append(pltpu.make_async_copy(up_ref.at[:, depth, :], wbuf.at[4 + s], ws.at[1, s]))
        gate_in[s].start()
        up_in[s].start()
    down_slot = (1, 4, 0, 8)
    pieces = width // hidden

    def fetch_down(s):
        for piece in range(pieces):
            start = pl.multiple_of((tp ^ s) * width + piece * hidden, hidden)
            copy = pltpu.make_async_copy(
                down_ref.at[:, :, pl.ds(start, hidden)],
                wbuf.at[down_slot[s], :, pl.ds(piece * hidden, hidden), :],
                ws.at[2 + piece, s],
            )
            copy.start()
            down_in[s, piece] = copy

    fetch_down(3)
    load("out_gain", out_gain_in, out_gain_v)
    load("out_proj", out_proj_in, out_proj_v)

    ids = ids_v[...]
    local_ids = ids & (GROUP - 1)
    group = jnp.right_shift(ids[0:1], GROUP.bit_length() - 1)
    offset = jnp.where(group >= plane, group - plane, group - plane + planes)
    in_group = lax.broadcasted_iota(jnp.int32, (8, tokens), 0) == offset
    names = lax.broadcasted_iota(jnp.int32, (planes * GROUP, tokens), 0)
    hit = [names == offset * GROUP + local_ids[k : k + 1] for k in range(2)]
    counted = jnp.concatenate(
        [in_group.astype(f32), hit[0].astype(f32) + hit[1].astype(f32)], axis=0
    ).astype(bf)
    before = (
        lax.broadcasted_iota(jnp.int32, (tokens, tokens), 0)
        < lax.broadcasted_iota(jnp.int32, (tokens, tokens), 1)
    ).astype(f32).astype(bf)
    earlier = jnp.dot(counted, before, preferred_element_type=f32)
    rank = jnp.sum(jnp.where(in_group, earlier[0:8], 0.0), axis=0, keepdims=True).astype(jnp.int32)
    codes = [
        local_ids[k : k + 1].astype(f32) * CAP
        + jnp.sum(jnp.where(hit[k], earlier[8:], 0.0), axis=0, keepdims=True)
        + 1.0
        for k in range(2)
    ]
    route = weights_v[...]
    route_high = route.astype(bf).astype(f32)
    route_low = route - route_high
    line = lax.broadcasted_iota(jnp.int32, (16, tokens), 0)
    meta = jnp.zeros((16, tokens), f32)
    meta_rows = codes + [route_high[0:1], route_high[1:2], route_low[0:1], route_low[1:2]]
    for i, row in enumerate(meta_rows):
        meta = jnp.where(line == i, row, meta)
    select = (
        lax.broadcasted_iota(jnp.int32, (planes * cap, tokens), 0) == offset * cap + rank
    ).astype(f32)
    select_b = select.astype(bf)
    wide = (
        lax.broadcasted_iota(jnp.int32, (planes * PAD, tokens), 0) == offset * PAD + rank
    ).astype(f32).astype(bf)
    meta_all = lax.dot_general(meta.astype(bf), wide, across, preferred_element_type=f32).astype(bf)
    for d in range(planes):
        metas_out[d] = meta_all[:, d * PAD : (d + 1) * PAD]
    metas[0, 0] = meta_all[:, 0:PAD]

    stream_f = stream_v[...].astype(f32)
    scale = lax.rsqrt(jnp.mean(stream_f * stream_f, axis=-1, keepdims=True) + EPS)
    own_cols = pl.ds(pl.multiple_of(tp * width, width), width)
    own_normed = (
        stream_v[:, own_cols].astype(f32) * scale * moe_gain_v[:, own_cols]
    ).astype(bf)
    out_rows = jnp.dot(select_b[cap:], own_normed, preferred_element_type=f32).astype(bf)
    for d in order:
        outgoing[d] = out_rows[(d - 1) * cap : d * cap]
    for d in order:
        send(outgoing.at[d], rows_ref.at[tp, 0, d], zs.at[3, d], zr.at[3, d], along(d))
        send(metas_out.at[d], metas.at[0, d], zs.at[2, d], zr.at[2, d], along(d))
    for q in range(4):
        cols = slice(q * width, (q + 1) * width)
        normed_q = (stream_v[:, cols].astype(f32) * scale * moe_gain_v[:, cols]).astype(bf)
        rows_ref[q, 0, 0] = jnp.dot(select_b[0:cap], normed_q, preferred_element_type=f32).astype(bf)
    send(rows_ref.at[:, 0, 0], rows_ref.at[:, 1, 0], ps.at[0, 0], pr.at[0, 0], partner)
    send(metas_out.at[0], metas.at[1, 0], ks.at[2, 0], kr.at[2, 0], partner)
    select_t[...] = jnp.transpose(select).astype(bf)

    def first(kind, d):
        if kind == 0:
            mine = latents.at[0, d, quarter(tp)]
            arrived(mine, zr.at[0, d], along(-d))
        else:
            mine = rows_ref.at[tp, 0, d]
            arrived(mine, zr.at[3, d], along(-d))
        send(mine, mine, xs.at[kind, 0, d], xr.at[kind, 0, d], near_x)
        send(mine, mine, xs.at[kind, 1, d], xr.at[kind, 1, d], near_y)
        if kind == 0:
            arrived(ropes.at[0, d], zr.at[1, d], along(-d))
            send(ropes.at[0, d], ropes.at[1, d], ks.at[1, d], kr.at[1, d], partner)
        else:
            send(mine, rows_ref.at[tp, 1, d], ps.at[0, d], pr.at[0, d], partner)
            arrived(metas.at[0, d], zr.at[2, d], along(-d))
            send(metas.at[0, d], metas.at[1, d], ks.at[2, d], kr.at[2, d], partner)

    def half_of(kind, flip, d, side):
        if kind == 0:
            start = (tp ^ flip) * quarter_rows + side * half_r
            return latents.at[0, d, pl.ds(pl.multiple_of(start, half_r), half_r)]
        return rows_ref.at[tp ^ flip, 0, d, :, halves[side]]

    def whole_of(kind, flip, d):
        if kind == 0:
            return latents.at[0, d, quarter(tp ^ flip)]
        return rows_ref.at[tp ^ flip, 0, d]

    def second(kind, d):
        arrived(whole_of(kind, 1, d), xr.at[kind, 0, d], near_x)
        piece = half_of(kind, 1, d, 0)
        send(piece, piece, xs.at[kind, 2, d], xr.at[kind, 2, d], near_y)
        arrived(whole_of(kind, 2, d), xr.at[kind, 1, d], near_y)
        piece = half_of(kind, 2, d, 1)
        send(piece, piece, xs.at[kind, 3, d], xr.at[kind, 3, d], near_x)
        if kind == 1:
            for flip in (1, 2):
                send(
                    rows_ref.at[tp ^ flip, 0, d],
                    rows_ref.at[tp ^ flip, 1, d],
                    ps.at[flip, d],
                    pr.at[flip, d],
                    partner,
                )

    def third(kind, d):
        arrived(half_of(kind, 3, d, 0), xr.at[kind, 2, d], near_y)
        arrived(half_of(kind, 3, d, 1), xr.at[kind, 3, d], near_x)
        if kind == 0:
            send(latents.at[0, d], latents.at[1, d], ks.at[0, d], kr.at[0, d], partner)
        else:
            mine = rows_ref.at[tp ^ 3, 0, d]
            send(mine, rows_ref.at[tp ^ 3, 1, d], ps.at[3, d], pr.at[3, d], partner)

    def run_steps(kind_steps):
        for stage, kind, d in kind_steps:
            (first, second, third)[stage - 1](kind, d)

    loads["queries"].wait()
    loads["query_gain"].wait()
    loads["key_gain"].wait()
    loads["table"].wait()
    half = ROPE // 2
    query_t = jnp.transpose(queries_v[...].astype(f32))
    gain_q = to_column(query_gain_v[...])
    gain_k = to_column(key_gain_v[...])
    own_lanes = pl.ds(pl.multiple_of(ep * tokens, tokens), tokens)
    cos_q, sin_q = table_v[0:half, own_lanes], table_v[half:ROPE, own_lanes]
    for h in range(head_count):
        z = query_t[h * QKD : (h + 1) * QKD]
        z = z * lax.rsqrt(jnp.mean(z * z, axis=0, keepdims=True) + EPS) * gain_q
        turned_a, turned_b = turn(z[NOPE : NOPE + half], z[NOPE + half :], cos_q, sin_q)
        turned_q[h] = jnp.concatenate([z[:NOPE], turned_a, turned_b], axis=0).astype(bf)

    run_steps([(1, 0, 1), (1, 0, 2), (2, 0, 1), (1, 0, 3), (2, 0, 2), (3, 0, 1)])
    run_steps([(1, 1, 1), (2, 0, 3), (3, 0, 2), (3, 0, 3)])

    for d in range(planes):
        arrived(latents.at[1, d], kr.at[0, d], partner)
        arrived(ropes.at[1, d], kr.at[1, d], partner)
    loads["key_up"].wait()
    loads["value_up"].wait()
    starts = [
        ((plane - d + planes) % planes * 2 + (core ^ parity)) * tokens
        for parity in range(2)
        for d in range(planes)
    ]
    key_total = blocks * tokens
    key_rows = latents[...].reshape(key_total, latents.shape[-1])
    key_t = lax.dot_general(
        key_up_v[...], key_rows, (((0,), (1,)), ((), ())), preferred_element_type=f32
    )
    key_t = key_t.astype(bf).astype(f32)
    values_v[...] = jnp.dot(key_rows, value_up_v[...], preferred_element_type=f32).astype(bf)
    run_steps([(1, 1, 2), (2, 1, 1)])
    rope_t = jnp.concatenate(
        [ropes[parity, d].astype(f32) for parity in range(2) for d in range(planes)], axis=1
    )
    lanes = [pl.ds(pl.multiple_of(start, tokens), tokens) for start in starts]
    cos_k = jnp.concatenate([table_v[0:half, lane] for lane in lanes], axis=1)
    sin_k = jnp.concatenate([table_v[half:ROPE, lane] for lane in lanes], axis=1)
    lane_ids = lax.broadcasted_iota(jnp.int32, (1, tokens), 1)
    key_pos = jnp.concatenate([lane_ids + start for start in starts], axis=1)
    query_pos = ep * tokens + lax.broadcasted_iota(jnp.int32, (tokens, 1), 0)
    visible = key_pos <= query_pos
    rope_squares = jnp.sum(rope_t * rope_t, axis=0, keepdims=True)
    for h in range(head_count):
        nope = key_t[h * NOPE : (h + 1) * NOPE]
        squares = jnp.sum(nope * nope, axis=0, keepdims=True) + rope_squares
        factor = lax.rsqrt(squares / QKD + EPS)
        nope = nope * factor * gain_k[:NOPE]
        spun = rope_t * factor * gain_k[NOPE:]
        turned_a, turned_b = turn(spun[:half], spun[half:], cos_k, sin_k)
        turned_k[h] = jnp.concatenate([nope, turned_a, turned_b], axis=0).astype(bf)
    head_of = jnp.right_shift(
        lax.broadcasted_iota(jnp.int32, (tokens, head_count * VDIM), 1), VDIM.bit_length() - 1
    )

    def attend(h, attn):
        scores = (
            lax.dot_general(turned_q[h], turned_k[h], turned, preferred_element_type=f32)
            * QKD ** (-0.5)
        )
        scores = jnp.where(visible, scores, -1e30)
        expo = jnp.exp(scores - jnp.max(scores, axis=-1, keepdims=True))
        total = jnp.sum(expo, axis=-1, keepdims=True)
        mixed_h = jnp.dot(expo.astype(bf), values_v[...], preferred_element_type=f32) / total
        return jnp.where(head_of == h, mixed_h, attn)

    attn = jnp.zeros((tokens, head_count * VDIM), f32)
    for h in range(head_count // 2):
        attn = attend(h, attn)
    run_steps([(1, 1, 3)])
    for h in range(head_count // 2, head_count):
        attn = attend(h, attn)
    heads[tp] = attn.astype(bf)
    run_steps([(2, 1, 2), (3, 1, 1)])

    for d in range(planes):
        arrived(metas.at[1, d], kr.at[2, d], partner)
    spot = (
        lax.broadcasted_iota(jnp.int32, (cap, PAD), 0)
        == lax.broadcasted_iota(jnp.int32, (cap, PAD), 1)
    ).astype(f32).astype(bf)
    info = jnp.concatenate(
        [
            lax.dot_general(spot, metas[parity, d], across, preferred_element_type=f32)
            for parity in range(2)
            for d in range(planes)
        ],
        axis=0,
    )
    info_b = info.astype(bf)
    block_of = jnp.concatenate(
        [jnp.full((cap, 1), block, jnp.int32) for block in range(blocks)], axis=0
    )
    slot_ids = lax.broadcasted_iota(jnp.int32, (row_total, slot_total), 1)
    place = jnp.zeros((row_total, slot_total), f32)
    placed_t = jnp.zeros((slot_total, row_total), f32)
    slot_weights = jnp.zeros((slot_total, 1), f32)
    for k in range(2):
        column = info[:, k : k + 1]
        code = column.astype(jnp.int32) - 1 - core * (experts * CAP)
        inside = (column > 0.5) & (code >= 0) & (code < experts * CAP)
        expert = jnp.zeros_like(code)
        for e in range(1, experts):
            expert += (code >= e * CAP).astype(jnp.int32)
        where = expert * (slots - CAP) + block_of * CAP + code
        match = (slot_ids == jnp.where(inside, where, -1)).astype(f32)
        match_t = jnp.transpose(match)
        place += match
        placed_t += match_t
        found = jnp.dot(match_t.astype(bf), info_b, preferred_element_type=f32)
        slot_weights += found[:, 2 + k : 3 + k] + found[:, 4 + k : 5 + k]
    place_v[...] = place.astype(bf)
    place_t[...] = placed_t.astype(bf)
    slot_w[...] = slot_weights
    run_steps([(2, 1, 3), (3, 1, 2)])
    for i, peer in enumerate((near_x, near_y, corner)):
        send(heads.at[tp], heads.at[tp], hs.at[i], hr.at[i], peer)

    def feed(s):
        for d in range(planes):
            if s == 0 and d == 0:
                arrived(rows_ref.at[:, 1, 0], pr.at[0, 0], partner)
            elif d > 0:
                arrived(rows_ref.at[tp ^ s, 1, d], pr.at[s, d], partner)
        rows = rows_ref[tp ^ s].reshape(row_total, width)
        taken[...] = jnp.dot(place_t[...], rows, preferred_element_type=f32).astype(bf)
        gate_in[s].wait()
        up_in[s].wait()
        for e in range(experts):
            mine = slice(e * slots, (e + 1) * slots)
            picked = taken[mine, :]
            gate = jnp.dot(picked, wbuf[s, e], preferred_element_type=f32)
            upper = jnp.dot(picked, wbuf[4 + s, e], preferred_element_type=f32)
            if s > 0:
                gate += gate_acc[e]
                upper += up_acc[e]
            if s < 3:
                gate_acc[e] = gate
                up_acc[e] = upper
            else:
                hidden_v[mine, :] = (
                    gate / (1.0 + jnp.exp(-gate)) * upper * slot_w[mine, :]
                ).astype(bf)

    feed(0)
    fetch_down(2)
    fetch_down(1)
    run_steps([(3, 1, 3)])
    feed(1)
    fetch_down(0)
    feed(2)
    feed(3)

    def spread(s):
        for piece in range(pieces):
            down_in[s, piece].wait()
        for e in range(experts):
            mine = slice(e * slots, (e + 1) * slots)
            for piece in range(pieces):
                cols = slice(piece * hidden, (piece + 1) * hidden)
                given[mine, cols] = jnp.dot(
                    hidden_v[mine, :], wbuf[down_slot[s], e, cols, :], preferred_element_type=f32
                ).astype(bf)
        summed = jnp.dot(place_v[...], given[...], preferred_element_type=f32).astype(bf)
        part[s] = summed.reshape(2, planes, cap, width)
        for d in range(planes):
            send(part.at[s, 1, d], other.at[s, d], cs.at[s, d], cr.at[s, d], partner)

    def join(s):
        for d in range(planes):
            arrived(other.at[s, d], cr.at[s, d], partner)
            part[s, 0, d] = (part[s, 0, d].astype(f32) + other[s, d].astype(f32)).astype(bf)

    away = order + [0]

    def start_rest(d):
        send(part.at[2, 0, d, :, high], by2.at[d, :, high], rs.at[2, d], rr.at[2, d], near_y)
        send(part.at[1, 0, d, :, low], bx2.at[d, :, low], rs.at[3, d], rr.at[3, d], near_x)

    def pass_on(d):
        arrived(bx1.at[d], rr.at[0, d], near_x)
        part[2, 0, d, :, low] = (
            part[2, 0, d, :, low].astype(f32) + bx1[d].astype(f32)
        ).astype(bf)
        send(part.at[2, 0, d, :, low], by2.at[d, :, low], rs.at[4, d], rr.at[4, d], near_y)
        arrived(by1.at[d], rr.at[1, d], near_y)
        part[1, 0, d, :, high] = (
            part[1, 0, d, :, high].astype(f32) + by1[d].astype(f32)
        ).astype(bf)
        send(part.at[1, 0, d, :, high], bx2.at[d, :, high], rs.at[5, d], rr.at[5, d], near_x)

    def finish(d):
        arrived(by2.at[d, :, high], rr.at[2, d], near_y)
        arrived(bx2.at[d, :, low], rr.at[3, d], near_x)
        arrived(by2.at[d, :, low], rr.at[4, d], near_y)
        arrived(bx2.at[d, :, high], rr.at[5, d], near_x)
        full = (
            part[0, 0, d].astype(f32) + bx2[d].astype(f32) + by2[d].astype(f32)
        ).astype(bf)
        if d == 0:
            back[0] = full
        else:
            done[d] = full
            send(done.at[d], back.at[d], bs.at[d], br.at[d], along(-d))

    spread(3)
    spread(2)
    join(3)
    for d in away:
        send(part.at[3, 0, d, :, low], bx1.at[d], rs.at[0, d], rr.at[0, d], near_x)
        send(part.at[3, 0, d, :, high], by1.at[d], rs.at[1, d], rr.at[1, d], near_y)
    spread(1)
    join(2)
    join(1)
    for d in order:
        start_rest(d)
    spread(0)
    for d in order:
        pass_on(d)
    start_rest(0)
    pass_on(0)
    join(0)

    for i, peer in enumerate((near_x, near_y, corner)):
        arrived(heads.at[tp ^ (i + 1)], hr.at[i], peer)
    loads["out_gain"].wait()
    loads["out_proj"].wait()
    block_f = jnp.concatenate([heads[q] for q in range(4)], axis=1).astype(f32)
    squares = jnp.mean(block_f * block_f, axis=-1, keepdims=True)
    scaled = (block_f * out_gain_v[...]).astype(bf)
    product = jnp.dot(scaled, out_proj_v[...], preferred_element_type=f32)
    mixed_ref[...] = (product * lax.rsqrt(squares + EPS)).astype(bf)

    for d in away:
        finish(d)
    for d in order:
        arrived(back.at[d], br.at[d], along(d))
    expert_ref[...] = jnp.dot(
        select_t[...], back[...].reshape(planes * cap, width), preferred_element_type=f32
    ).astype(bf)
    for copy in sent:
        copy.wait_send()


def fused(
    queries,
    kv_latent,
    rope_key,
    latent_gain,
    key_up,
    value_up,
    query_gain,
    key_gain,
    out_gain,
    out_proj,
    moe_input,
    moe_gain,
    expert_ids,
    route_weights,
    w_gate,
    w_up,
    w_down,
):
    f32, bf, i32 = jnp.float32, jnp.bfloat16, jnp.int32
    planes = lax.axis_size("ep") // 2
    tokens, model = moe_input.shape
    width = model // lax.axis_size("tp")
    experts, _, hidden = w_gate.shape
    cap = group_cap()
    blocks = 2 * planes
    row_total, slots = blocks * cap, blocks * CAP
    slot_total = experts * slots
    rank = kv_latent.shape[1]
    head_count = key_up.shape[1] // NOPE
    total = tokens * lax.axis_size("ep")
    v_cols = value_up.shape[1]
    table = jnp.asarray(rope_table(total))
    dma = pltpu.SemaphoreType.DMA
    vmem = pltpu.VMEM
    operands = (
        queries,
        kv_latent,
        rope_key.T,
        latent_gain.reshape(1, -1),
        key_up,
        value_up,
        query_gain.reshape(1, -1),
        key_gain.reshape(1, -1),
        out_gain.reshape(1, -1),
        out_proj,
        moe_input,
        moe_gain.reshape(1, -1),
        expert_ids.T,
        route_weights.T,
        w_gate,
        w_up,
        w_down,
        table,
    )
    mixed, expert_out = pl.pallas_call(
        functools.partial(layer_kernel, planes),
        out_shape=(
            jax.ShapeDtypeStruct((tokens, out_proj.shape[1]), bf),
            jax.ShapeDtypeStruct((tokens, width), bf),
        ),
        in_specs=[pl.BlockSpec(memory_space=pl.ANY)] * len(operands),
        out_specs=(pl.BlockSpec(memory_space=pltpu.VMEM),) * 2,
        scratch_shapes=[
            vmem(queries.shape, bf),
            vmem(kv_latent.shape, bf),
            vmem((1, rank), f32),
            vmem(key_up.shape, bf),
            vmem(value_up.shape, bf),
            vmem((1, QKD), f32),
            vmem((1, QKD), f32),
            vmem((1, out_gain.shape[0]), f32),
            vmem(out_proj.shape, bf),
            vmem(moe_input.shape, bf),
            vmem((1, model), f32),
            vmem((2, tokens), i32),
            vmem((2, tokens), f32),
            vmem(table.shape, f32),
            vmem((9, experts, width, hidden), bf),
            vmem((2, planes, tokens, rank), bf),
            vmem((2, planes, ROPE, tokens), bf),
            vmem((planes, cap, width), bf),
            vmem((planes, 16, PAD), bf),
            vmem((4, 2, planes, cap, width), bf),
            vmem((2, planes, 16, PAD), bf),
            vmem((head_count, QKD, tokens), bf),
            vmem((head_count, QKD, total), bf),
            vmem((total, v_cols), bf),
            vmem((4, tokens, v_cols), bf),
            vmem((tokens, planes * cap), bf),
            vmem((row_total, slot_total), bf),
            vmem((slot_total, row_total), bf),
            vmem((slot_total, 1), f32),
            vmem((slot_total, width), bf),
            vmem((experts, slots, hidden), f32),
            vmem((experts, slots, hidden), f32),
            vmem((slot_total, hidden), bf),
            vmem((slot_total, width), bf),
            vmem((4, 2, planes, cap, width), bf),
            vmem((4, planes, cap, width), bf),
            vmem((planes, cap, width // 2), bf),
            vmem((planes, cap, width // 2), bf),
            vmem((planes, cap, width), bf),
            vmem((planes, cap, width), bf),
            vmem((planes, cap, width), bf),
            vmem((planes, cap, width), bf),
            dma((15,)),
            dma((4, 4)),
            dma((4, planes)),
            dma((4, planes)),
            dma((2, 4, planes)),
            dma((2, 4, planes)),
            dma((3, planes)),
            dma((3, planes)),
            dma((4, planes)),
            dma((4, planes)),
            dma((3,)),
            dma((3,)),
            dma((4, planes)),
            dma((4, planes)),
            dma((6, planes)),
            dma((6, planes)),
            dma((planes,)),
            dma((planes,)),
        ],
        compiler_params=pltpu.CompilerParams(
            collective_id=0, has_side_effects=True, vmem_limit_bytes=67043328
        ),
        name="layer",
    )(*operands)
    return (mixed, expert_out)


def layer(*arrays):
    gate, stream = arrays[14], arrays[10]
    tp_count, ep_count = lax.axis_size("tp"), lax.axis_size("ep")
    fits = (
        tp_count == 4
        and ep_count % 2 == 0
        and ep_count // 2 <= GROUP
        and 2 * gate.shape[0] == GROUP
        and stream.shape[0] == PAD
        and stream.shape[1] // tp_count == 2 * gate.shape[2]
    )
    return fused(*arrays) if fits else shards(*arrays)


def solution(mesh):
    in_specs = (
        P("ep", "tp"),
        P("ep", None),
        P("ep", None),
        P(),
        P(None, "tp"),
        P(None, "tp"),
        P(),
        P(),
        P(),
        P(None, "tp"),
        P("ep", None),
        P(),
        P("ep", None),
        P("ep", None),
        P("ep", None, "tp"),
        P("ep", None, "tp"),
        P("ep", "tp", None),
    )
    out_specs = (P("ep", "tp"), P("ep", "tp"))
    return jax.shard_map(layer, mesh=mesh, in_specs=in_specs, out_specs=out_specs, check_vma=False)
```

```python
import functools

import jax
import jax.numpy as jnp
import numpy as np
from jax import lax
from jax.experimental import pallas as pl
from jax.experimental.pallas import tpu as pltpu
from jax.sharding import PartitionSpec as P

NOPE = 64
ROPE = 32
VDIM = 64
QKD = 96
CAP = 12


EPS = 1e-06
THETA = 10000.0


def rotate_half(values_in, positions):
    half_width = ROPE // 2
    inverse = THETA ** (-jnp.arange(half_width, dtype=jnp.float32) / half_width)
    angles = positions.astype(jnp.float32)[:, None] * inverse
    cosine = jnp.cos(angles)[:, None, :]
    sine = jnp.sin(angles)[:, None, :]
    first_half = values_in[..., :half_width]
    second_half = values_in[..., half_width:]
    return jnp.concatenate(
        [first_half * cosine - second_half * sine, second_half * cosine + first_half * sine],
        axis=-1,
    )


def head_norm(values_in, gain_vec):
    return (
        values_in
        * lax.rsqrt(jnp.mean(values_in * values_in, axis=-1, keepdims=True) + EPS)
        * gain_vec
    )


def make_queries(queries, query_gain, positions):
    row_count = queries.shape[0]
    head_count = queries.shape[1] // QKD
    normed = head_norm(queries.astype(jnp.float32).reshape(row_count, head_count, QKD), query_gain)
    turned = jnp.concatenate(
        [normed[..., :NOPE], rotate_half(normed[..., NOPE:], positions)], axis=-1
    )
    return turned.astype(jnp.bfloat16)


def make_keys(latent, rope_part, latent_gain, key_up, value_up, key_gain, positions):
    row_count = latent.shape[0]
    head_count = key_up.shape[1] // NOPE
    latent_f = latent.astype(jnp.float32)
    latent_n = (
        latent_f
        * lax.rsqrt(jnp.mean(latent_f * latent_f, axis=-1, keepdims=True) + EPS)
        * latent_gain
    ).astype(jnp.bfloat16)
    key_nope = jnp.dot(latent_n, key_up, preferred_element_type=jnp.float32).astype(jnp.bfloat16)
    key_nope = lax.optimization_barrier(key_nope)
    value_rows = jnp.dot(latent_n, value_up, preferred_element_type=jnp.float32).astype(
        jnp.bfloat16
    )
    shared = jnp.broadcast_to(
        rope_part.astype(jnp.float32)[:, None, :], (row_count, head_count, ROPE)
    )
    key_full = jnp.concatenate(
        [key_nope.astype(jnp.float32).reshape(row_count, head_count, NOPE), shared], axis=-1
    )
    normed = head_norm(key_full, key_gain)
    turned = jnp.concatenate(
        [normed[..., :NOPE], rotate_half(normed[..., NOPE:], positions)], axis=-1
    )
    return (turned.astype(jnp.bfloat16), value_rows.reshape(row_count, head_count, VDIM))


def shards(
    queries,
    kv_latent,
    rope_key,
    latent_gain,
    key_up,
    value_up,
    query_gain,
    key_gain,
    out_gain,
    out_proj,
    moe_input,
    moe_gain,
    expert_ids,
    route_weights,
    w_gate,
    w_up,
    w_down,
):
    tok_rows = queries.shape[0]
    head_count = key_up.shape[1] // NOPE
    query_pos = lax.axis_index("ep") * tok_rows + jnp.arange(tok_rows, dtype=jnp.int32)
    query_rot = make_queries(queries, query_gain, query_pos)
    inv_scale = QKD ** (-0.5)
    blocks_in = (
        lax.all_gather(kv_latent, "ep", axis=0, tiled=True),
        lax.all_gather(rope_key, "ep", axis=0, tiled=True),
    )
    key_pos = jnp.arange(blocks_in[0].shape[0], dtype=jnp.int32)
    key_rot, value_rows = make_keys(
        blocks_in[0], blocks_in[1], latent_gain, key_up, value_up, key_gain, key_pos
    )
    top_prev = jnp.full((head_count, tok_rows), -1e30, jnp.float32)
    key_pos = jnp.arange(key_rot.shape[0], dtype=jnp.int32)
    scores = (
        jnp.einsum("qhd,khd->hqk", query_rot, key_rot, preferred_element_type=jnp.float32)
        * inv_scale
    )
    visible = key_pos[None, :] <= query_pos[:, None]
    scores = jnp.where(visible[None], scores, -1e30)
    top_new = jnp.maximum(top_prev, jnp.max(scores, axis=-1))
    expo = jnp.exp(scores - top_new[..., None])
    total_new = jnp.sum(expo, axis=-1)
    accum_new = jnp.einsum(
        "hqk,khd->hqd", expo.astype(jnp.bfloat16), value_rows, preferred_element_type=jnp.float32
    )
    attn = (accum_new / total_new[..., None]).astype(jnp.bfloat16)
    attn = attn.transpose(1, 0, 2).reshape(tok_rows, head_count * VDIM)
    block_f = lax.all_gather(attn, "tp", axis=1, tiled=True).astype(jnp.float32)
    scaled = (block_f * out_gain[None, :]).astype(jnp.bfloat16)
    product = jnp.dot(scaled, out_proj, preferred_element_type=jnp.float32)
    product, squares = (product, jnp.sum(block_f * block_f, axis=-1))
    mixed = (product * lax.rsqrt(squares / out_gain.shape[0] + EPS)[:, None]).astype(jnp.bfloat16)
    row_count = moe_input.shape[0]
    top_count = expert_ids.shape[1]
    local_experts = w_gate.shape[0]
    ep_count = lax.axis_size("ep")
    expert_count = local_experts * ep_count
    stream_f = moe_input.astype(jnp.float32)
    normed = (
        stream_f * lax.rsqrt(jnp.mean(stream_f * stream_f, axis=-1, keepdims=True) + EPS) * moe_gain
    ).astype(jnp.bfloat16)
    flat_ids = expert_ids.reshape(-1)
    onehot = (flat_ids[:, None] == jnp.arange(expert_count, dtype=jnp.int32)[None, :]).astype(
        jnp.int32
    )
    slot_rank = jnp.sum((jnp.cumsum(onehot, axis=0) - onehot) * onehot, axis=1)
    slot_index = flat_ids * CAP + slot_rank
    token_index = jnp.arange(row_count * top_count, dtype=jnp.int32) // top_count
    slot_token = jnp.zeros((expert_count * CAP,), jnp.int32).at[slot_index].set(token_index)
    slot_used = jnp.zeros((expert_count * CAP,), jnp.bool_).at[slot_index].set(True)
    outgoing = jnp.where(slot_used[:, None], normed[slot_token], jnp.zeros((), jnp.bfloat16))
    outgoing = outgoing.reshape(ep_count, local_experts, CAP, normed.shape[1])
    piece_width = normed.shape[1] // lax.axis_size("tp")
    my_columns = lax.dynamic_slice_in_dim(
        outgoing, lax.axis_index("tp") * piece_width, piece_width, 3
    )
    arrived_part = lax.all_to_all(my_columns, "ep", split_axis=0, concat_axis=0, tiled=True)
    piece = lax.all_gather(arrived_part, "tp", axis=3, tiled=True)
    gate_acc = jnp.einsum("secd,edf->secf", piece, w_gate, preferred_element_type=jnp.float32)
    upper_acc = jnp.einsum("secd,edf->secf", piece, w_up, preferred_element_type=jnp.float32)
    hidden = (jax.nn.silu(gate_acc) * upper_acc).astype(jnp.bfloat16)
    out_cols = w_down.shape[2] // lax.axis_size("tp")
    term = jnp.einsum("secf,efd->dsec", hidden, w_down, preferred_element_type=jnp.float32)
    summed = lax.psum_scatter(
        term.reshape(lax.axis_size("tp") * out_cols, -1).astype(jnp.bfloat16),
        "tp",
        scatter_dimension=0,
        tiled=True,
    )
    expert_y = summed.T.reshape(ep_count, local_experts * CAP, out_cols)
    returned_rows = lax.all_to_all(expert_y, "ep", split_axis=0, concat_axis=0, tiled=True).reshape(
        expert_count * CAP, out_cols
    )
    picked = returned_rows[slot_index].reshape(row_count, top_count, out_cols).astype(jnp.float32)
    expert_out = jnp.sum(picked * route_weights[..., None], axis=1).astype(jnp.bfloat16)
    return (mixed, expert_out)


MESH = pl.DeviceIdType.MESH
GROUP = 8
PAD = 128


def group_cap():
    return GROUP * CAP // 2


def rdma(src, dst, send_sem, recv_sem, device):
    copy = pltpu.make_async_remote_copy(
        src_ref=src,
        dst_ref=dst,
        send_sem=send_sem,
        recv_sem=recv_sem,
        device_id=device,
        device_id_type=MESH,
    )
    copy.start()
    return copy


def arrived(dst, sem, device):
    pltpu.make_async_remote_copy(
        src_ref=dst,
        dst_ref=dst,
        send_sem=sem,
        recv_sem=sem,
        device_id=device,
        device_id_type=MESH,
    ).wait_recv()


def places(planes):
    ep = lax.axis_index("ep")
    tp = lax.axis_index("tp")
    plane = ep // 2
    core = ep % 2

    def along(offset):
        return (lax.rem(plane + offset + planes, planes) * 2 + core, tp)

    partner = (plane * 2 + 1 - core, tp)
    near_x = (ep, tp ^ 1)
    near_y = (ep, tp ^ 2)
    corner = (ep, tp ^ 3)
    return tp, along, partner, near_x, near_y, corner


def greet(peers):
    barrier = pltpu.get_barrier_semaphore()
    for peer in peers:
        pl.semaphore_signal(barrier, inc=1, device_id=peer, device_id_type=MESH)
    pl.semaphore_wait(barrier, len(peers))


def rope_table(total):
    half = ROPE // 2
    inverse = np.float32(THETA) ** (-np.arange(half, dtype=np.float32) / np.float32(half))
    angles = np.arange(total, dtype=np.float32)[None, :] * inverse[:, None]
    return np.concatenate([np.cos(angles), np.sin(angles)], axis=0).astype(np.float32)


def turn(first_half, second_half, cosine, sine):
    return (
        first_half * cosine - second_half * sine,
        second_half * cosine + first_half * sine,
    )


def to_column(row):
    size = row.shape[1]
    rows = lax.broadcasted_iota(jnp.int32, (size, size), 0)
    cols = lax.broadcasted_iota(jnp.int32, (size, size), 1)
    return jnp.sum(jnp.where(rows == cols, row, 0.0), axis=1, keepdims=True)


def layer_kernel(
    planes,
    queries_in,
    latent_in,
    rope_in,
    latent_gain_in,
    key_up_in,
    value_up_in,
    query_gain_in,
    key_gain_in,
    out_gain_in,
    out_proj_in,
    stream_in,
    moe_gain_in,
    ids_in,
    weights_in,
    gate_ref,
    up_ref,
    down_ref,
    table_in,
    mixed_ref,
    expert_ref,
    queries_v,
    latent_v,
    latent_gain_v,
    key_up_v,
    value_up_v,
    query_gain_v,
    key_gain_v,
    out_gain_v,
    out_proj_v,
    stream_v,
    moe_gain_v,
    ids_v,
    weights_v,
    table_v,
    wbuf,
    latents,
    ropes,
    outgoing,
    metas_out,
    rows_ref,
    metas,
    turned_q,
    turned_k,
    values_v,
    heads,
    select_t,
    place_v,
    place_t,
    slot_w,
    taken,
    gate_acc,
    up_acc,
    hidden_v,
    given,
    part,
    other,
    bx1,
    by1,
    bx2,
    by2,
    done,
    back,
    loc,
    ws,
    zs,
    zr,
    xs,
    xr,
    ks,
    kr,
    ps,
    pr,
    hs,
    hr,
    cs,
    cr,
    rs,
    rr,
    bs,
    br,
):
    f32, bf = jnp.float32, jnp.bfloat16
    ep = lax.axis_index("ep")
    plane, core = ep // 2, ep % 2
    tp, along, partner, near_x, near_y, corner = places(planes)
    peers = [along(d) for d in range(1, planes)] + [partner, near_x, near_y, corner]
    barrier = pltpu.get_barrier_semaphore()
    for peer in peers:
        pl.semaphore_signal(barrier, inc=1, device_id=peer, device_id_type=MESH)

    blocks = 2 * planes
    tokens, model = stream_in.shape
    cap, width = outgoing.shape[1], outgoing.shape[2]
    experts, hidden = gate_ref.shape[0], gate_ref.shape[2]
    row_total, slots = blocks * cap, blocks * CAP
    slot_total = experts * slots
    quarter_rows = tokens // 4
    half_r, half_w = quarter_rows // 2, width // 2
    low, high = pl.ds(0, half_w), pl.ds(half_w, half_w)
    halves = (low, high)
    head_count = key_up_in.shape[1] // NOPE
    order = sorted(range(1, planes), key=lambda d: (min(d, planes - d), d))
    away = sorted(range(1, planes), key=lambda d: (-min(d, planes - d), d)) + [0]
    turned = (((0,), (0,)), ((), ()))
    across = (((1,), (1,)), ((), ()))

    loads = {}

    def load(name, source, target):
        copy = pltpu.make_async_copy(source, target, loc.at[len(loads)])
        copy.start()
        loads[name] = copy

    load("ids", ids_in, ids_v)
    load("weights", weights_in, weights_v)
    load("stream", stream_in, stream_v)
    load("moe_gain", moe_gain_in, moe_gain_v)
    load("latent", latent_in, latent_v)
    load("latent_gain", latent_gain_in, latent_gain_v)
    load("rope", rope_in, ropes.at[0, 0])
    load("queries", queries_in, queries_v)
    load("query_gain", query_gain_in, query_gain_v)
    load("key_gain", key_gain_in, key_gain_v)
    load("table", table_in, table_v)
    load("key_up", key_up_in, key_up_v)
    load("value_up", value_up_in, value_up_v)

    sent = []

    def send(src, dst, send_sem, recv_sem, device):
        sent.append(rdma(src, dst, send_sem, recv_sem, device))

    def quarter(which):
        return pl.ds(pl.multiple_of(which * quarter_rows, quarter_rows), quarter_rows)

    loads["ids"].wait()
    loads["weights"].wait()
    ids = ids_v[...]
    local_ids = ids & (GROUP - 1)
    group = jnp.right_shift(ids[0:1], GROUP.bit_length() - 1)
    offset = jnp.where(group >= plane, group - plane, group - plane + planes)
    in_group = lax.broadcasted_iota(jnp.int32, (8, tokens), 0) == offset
    names = lax.broadcasted_iota(jnp.int32, (planes * GROUP, tokens), 0)
    hit = [names == offset * GROUP + local_ids[k : k + 1] for k in range(2)]
    counted = jnp.concatenate(
        [in_group.astype(f32), hit[0].astype(f32) + hit[1].astype(f32)], axis=0
    ).astype(bf)
    before = (
        lax.broadcasted_iota(jnp.int32, (tokens, tokens), 0)
        < lax.broadcasted_iota(jnp.int32, (tokens, tokens), 1)
    ).astype(f32).astype(bf)
    earlier = jnp.dot(counted, before, preferred_element_type=f32)
    rank = jnp.sum(jnp.where(in_group, earlier[0:8], 0.0), axis=0, keepdims=True).astype(jnp.int32)
    codes = [
        local_ids[k : k + 1].astype(f32) * CAP
        + jnp.sum(jnp.where(hit[k], earlier[8:], 0.0), axis=0, keepdims=True)
        + 1.0
        for k in range(2)
    ]
    route = weights_v[...]
    route_high = route.astype(bf).astype(f32)
    route_low = route - route_high
    line = lax.broadcasted_iota(jnp.int32, (16, tokens), 0)
    meta = jnp.zeros((16, tokens), f32)
    meta_rows = codes + [route_high[0:1], route_high[1:2], route_low[0:1], route_low[1:2]]
    for i, row in enumerate(meta_rows):
        meta = jnp.where(line == i, row, meta)
    select = (
        lax.broadcasted_iota(jnp.int32, (planes * cap, tokens), 0) == offset * cap + rank
    ).astype(f32)
    select_b = select.astype(bf)
    wide = (
        lax.broadcasted_iota(jnp.int32, (planes * PAD, tokens), 0) == offset * PAD + rank
    ).astype(f32).astype(bf)
    meta_all = lax.dot_general(meta.astype(bf), wide, across, preferred_element_type=f32).astype(bf)
    for d in range(planes):
        metas_out[d] = meta_all[:, d * PAD : (d + 1) * PAD]
    metas[0, 0] = meta_all[:, 0:PAD]

    loads["stream"].wait()
    loads["moe_gain"].wait()
    gate_in, up_in, down_in = [], [], {}
    for s in range(4):
        depth = pl.ds(pl.multiple_of((tp ^ s) * width, width), width)
        gate_in.append(
            pltpu.make_async_copy(gate_ref.at[:, depth, :], wbuf.at[s], ws.at[0, s])
        )
        up_in.append(pltpu.make_async_copy(up_ref.at[:, depth, :], wbuf.at[4 + s], ws.at[1, s]))
        gate_in[s].start()
        up_in[s].start()
    down_slot = (1, 4, 0, 8)
    pieces = width // hidden

    def fetch_down(s):
        for piece in range(pieces):
            start = pl.multiple_of((tp ^ s) * width + piece * hidden, hidden)
            copy = pltpu.make_async_copy(
                down_ref.at[:, :, pl.ds(start, hidden)],
                wbuf.at[down_slot[s], :, pl.ds(piece * hidden, hidden), :],
                ws.at[2 + piece, s],
            )
            copy.start()
            down_in[s, piece] = copy

    fetch_down(3)
    load("out_gain", out_gain_in, out_gain_v)
    load("out_proj", out_proj_in, out_proj_v)

    stream_f = stream_v[...].astype(f32)
    scale = lax.rsqrt(jnp.mean(stream_f * stream_f, axis=-1, keepdims=True) + EPS)
    own_cols = pl.ds(pl.multiple_of(tp * width, width), width)
    own_normed = (
        stream_v[:, own_cols].astype(f32) * scale * moe_gain_v[:, own_cols]
    ).astype(bf)
    out_rows = jnp.dot(select_b[cap:], own_normed, preferred_element_type=f32).astype(bf)
    for d in order:
        outgoing[d] = out_rows[(d - 1) * cap : d * cap]
    pl.semaphore_wait(barrier, len(peers))
    for d in order:
        send(outgoing.at[d], rows_ref.at[tp, 0, d], zs.at[3, d], zr.at[3, d], along(d))
        send(metas_out.at[d], metas.at[0, d], zs.at[2, d], zr.at[2, d], along(d))
    for q in range(4):
        cols = slice(q * width, (q + 1) * width)
        normed_q = (stream_v[:, cols].astype(f32) * scale * moe_gain_v[:, cols]).astype(bf)
        rows_ref[q, 0, 0] = jnp.dot(select_b[0:cap], normed_q, preferred_element_type=f32).astype(bf)
    send(rows_ref.at[:, 0, 0], rows_ref.at[:, 1, 0], ps.at[0, 0], pr.at[0, 0], partner)
    send(metas_out.at[0], metas.at[1, 0], ks.at[2, 0], kr.at[2, 0], partner)
    loads["latent"].wait()
    loads["latent_gain"].wait()
    latent_f = latent_v[...].astype(f32)
    latents[0, 0] = (
        latent_f
        * lax.rsqrt(jnp.mean(latent_f * latent_f, axis=-1, keepdims=True) + EPS)
        * latent_gain_v[...]
    ).astype(bf)
    loads["rope"].wait()
    select_t[...] = jnp.transpose(select).astype(bf)

    def first(kind, d):
        if kind == 0:
            mine = latents.at[0, d, quarter(tp)]
            arrived(mine, zr.at[0, d], along(-d))
        else:
            mine = rows_ref.at[tp, 0, d]
            arrived(mine, zr.at[3, d], along(-d))
        send(mine, mine, xs.at[kind, 0, d], xr.at[kind, 0, d], near_x)
        send(mine, mine, xs.at[kind, 1, d], xr.at[kind, 1, d], near_y)
        if kind == 0:
            arrived(ropes.at[0, d], zr.at[1, d], along(-d))
            send(ropes.at[0, d], ropes.at[1, d], ks.at[1, d], kr.at[1, d], partner)
        else:
            send(mine, rows_ref.at[tp, 1, d], ps.at[0, d], pr.at[0, d], partner)
            arrived(metas.at[0, d], zr.at[2, d], along(-d))
            send(metas.at[0, d], metas.at[1, d], ks.at[2, d], kr.at[2, d], partner)

    def half_of(kind, flip, d, side):
        if kind == 0:
            start = (tp ^ flip) * quarter_rows + side * half_r
            return latents.at[0, d, pl.ds(pl.multiple_of(start, half_r), half_r)]
        return rows_ref.at[tp ^ flip, 0, d, :, halves[side]]

    def whole_of(kind, flip, d):
        if kind == 0:
            return latents.at[0, d, quarter(tp ^ flip)]
        return rows_ref.at[tp ^ flip, 0, d]

    def second(kind, d):
        arrived(whole_of(kind, 1, d), xr.at[kind, 0, d], near_x)
        piece = half_of(kind, 1, d, 0)
        send(piece, piece, xs.at[kind, 2, d], xr.at[kind, 2, d], near_y)
        arrived(whole_of(kind, 2, d), xr.at[kind, 1, d], near_y)
        piece = half_of(kind, 2, d, 1)
        send(piece, piece, xs.at[kind, 3, d], xr.at[kind, 3, d], near_x)
        if kind == 1:
            for flip in (1, 2):
                send(
                    rows_ref.at[tp ^ flip, 0, d],
                    rows_ref.at[tp ^ flip, 1, d],
                    ps.at[flip, d],
                    pr.at[flip, d],
                    partner,
                )

    def third(kind, d):
        arrived(half_of(kind, 3, d, 0), xr.at[kind, 2, d], near_y)
        arrived(half_of(kind, 3, d, 1), xr.at[kind, 3, d], near_x)
        if kind == 0:
            send(latents.at[0, d], latents.at[1, d], ks.at[0, d], kr.at[0, d], partner)
        else:
            mine = rows_ref.at[tp ^ 3, 0, d]
            send(mine, rows_ref.at[tp ^ 3, 1, d], ps.at[3, d], pr.at[3, d], partner)

    loads["queries"].wait()
    loads["query_gain"].wait()
    loads["key_gain"].wait()
    loads["table"].wait()
    half = ROPE // 2
    query_t = jnp.transpose(queries_v[...].astype(f32))
    gain_q = to_column(query_gain_v[...])
    gain_k = to_column(key_gain_v[...])
    own_lanes = pl.ds(pl.multiple_of(ep * tokens, tokens), tokens)
    cos_q, sin_q = table_v[0:half, own_lanes], table_v[half:ROPE, own_lanes]
    for h in range(head_count):
        z = query_t[h * QKD : (h + 1) * QKD]
        z = z * lax.rsqrt(jnp.mean(z * z, axis=0, keepdims=True) + EPS) * gain_q
        turned_a, turned_b = turn(z[NOPE : NOPE + half], z[NOPE + half :], cos_q, sin_q)
        turned_q[h] = jnp.concatenate([z[:NOPE], turned_a, turned_b], axis=0).astype(bf)

    each = planes * CAP

    def both(ref, e):
        mine = slice(e * each, (e + 1) * each)
        return jnp.concatenate([ref[0, mine, :], ref[1, mine, :]], axis=0)

    def feed(s):
        for d in range(planes):
            if s == 0 and d == 0:
                arrived(rows_ref.at[:, 1, 0], pr.at[0, 0], partner)
            elif d > 0:
                arrived(rows_ref.at[tp ^ s, 1, d], pr.at[s, d], partner)
        for parity in range(2):
            rows = rows_ref[tp ^ s, parity].reshape(planes * cap, width)
            taken[parity] = jnp.dot(
                place_t[parity], rows, preferred_element_type=f32
            ).astype(bf)
        gate_in[s].wait()
        up_in[s].wait()
        for e in range(experts):
            picked = both(taken, e)
            gate = jnp.dot(picked, wbuf[s, e], preferred_element_type=f32)
            upper = jnp.dot(picked, wbuf[4 + s, e], preferred_element_type=f32)
            if s > 0:
                gate += gate_acc[e]
                upper += up_acc[e]
            if s < 3:
                gate_acc[e] = gate
                up_acc[e] = upper
            else:
                act = (gate / (1.0 + jnp.exp(-gate)) * upper * both(slot_w, e)).astype(bf)
                for parity in range(2):
                    hidden_v[parity, e * each : (e + 1) * each] = act[
                        parity * each : (parity + 1) * each
                    ]

    first(1, order[0])
    first(1, order[1])
    second(1, order[0])
    first(1, order[2])
    own_part = latents.at[0, 0, quarter(tp)]
    for d in order:
        send(own_part, latents.at[0, d, quarter(tp)], zs.at[0, d], zr.at[0, d], along(d))
        send(ropes.at[0, 0], ropes.at[0, d], zs.at[1, d], zr.at[1, d], along(d))
    send(latents.at[0, 0], latents.at[1, 0], ks.at[0, 0], kr.at[0, 0], partner)
    send(ropes.at[0, 0], ropes.at[1, 0], ks.at[1, 0], kr.at[1, 0], partner)

    second(1, order[1])
    for d in range(planes):
        arrived(metas.at[1, d], kr.at[2, d], partner)
    spot = (
        lax.broadcasted_iota(jnp.int32, (cap, PAD), 0)
        == lax.broadcasted_iota(jnp.int32, (cap, PAD), 1)
    ).astype(f32).astype(bf)
    side_rows, side_slots = planes * cap, experts * planes * CAP
    plane_of = jnp.concatenate(
        [jnp.full((cap, 1), d, jnp.int32) for d in range(planes)], axis=0
    )
    slot_ids = lax.broadcasted_iota(jnp.int32, (side_rows, side_slots), 1)
    for parity in range(2):
        info = jnp.concatenate(
            [
                lax.dot_general(spot, metas[parity, d], across, preferred_element_type=f32)
                for d in range(planes)
            ],
            axis=0,
        )
        info_b = info.astype(bf)
        place = jnp.zeros((side_rows, side_slots), f32)
        placed_t = jnp.zeros((side_slots, side_rows), f32)
        slot_weights = jnp.zeros((side_slots, 1), f32)
        for k in range(2):
            column = info[:, k : k + 1]
            code = column.astype(jnp.int32) - 1 - core * (experts * CAP)
            inside = (column > 0.5) & (code >= 0) & (code < experts * CAP)
            expert = jnp.zeros_like(code)
            for e in range(1, experts):
                expert += (code >= e * CAP).astype(jnp.int32)
            where = expert * ((planes - 1) * CAP) + plane_of * CAP + code
            match = (slot_ids == jnp.where(inside, where, -1)).astype(f32)
            match_t = jnp.transpose(match)
            place += match
            placed_t += match_t
            found = jnp.dot(match_t.astype(bf), info_b, preferred_element_type=f32)
            slot_weights += found[:, 2 + k : 3 + k] + found[:, 4 + k : 5 + k]
        place_v[parity] = place.astype(bf)
        place_t[parity] = placed_t.astype(bf)
        slot_w[parity] = slot_weights
    feed(0)
    fetch_down(2)
    fetch_down(1)
    second(1, order[-1])
    for d in order[:-1]:
        third(1, d)
    for d in order:
        first(0, d)
    feed(1)
    fetch_down(0)
    third(1, order[-1])
    for d in order[:-1]:
        second(0, d)
    feed(2)
    second(0, order[-1])
    feed(3)
    def spread(s):
        for piece in range(pieces):
            down_in[s, piece].wait()
        for e in range(experts):
            act = both(hidden_v, e)
            for piece in range(pieces):
                cols = slice(piece * hidden, (piece + 1) * hidden)
                result = jnp.dot(
                    act, wbuf[down_slot[s], e, cols, :], preferred_element_type=f32
                ).astype(bf)
                for parity in range(2):
                    given[parity, e * each : (e + 1) * each, cols] = result[
                        parity * each : (parity + 1) * each
                    ]
        for parity in (1, 0):
            summed = jnp.dot(place_v[parity], given[parity], preferred_element_type=f32).astype(bf)
            part[s, parity] = summed.reshape(planes, cap, width)
        for d in range(planes):
            send(part.at[s, 1, d], other.at[s, d], cs.at[s, d], cr.at[s, d], partner)

    def join(s, d):
        arrived(other.at[s, d], cr.at[s, d], partner)
        part[s, 0, d] = (part[s, 0, d].astype(f32) + other[s, d].astype(f32)).astype(bf)

    def start(d):
        send(part.at[3, 0, d, :, low], bx1.at[d], rs.at[0, d], rr.at[0, d], near_x)
        send(part.at[3, 0, d, :, high], by1.at[d], rs.at[1, d], rr.at[1, d], near_y)

    def rest_y(d):
        send(part.at[2, 0, d, :, high], by2.at[d, :, high], rs.at[2, d], rr.at[2, d], near_y)

    def rest_x(d):
        send(part.at[1, 0, d, :, low], bx2.at[d, :, low], rs.at[3, d], rr.at[3, d], near_x)

    def pass_on(d):
        arrived(bx1.at[d], rr.at[0, d], near_x)
        part[2, 0, d, :, low] = (
            part[2, 0, d, :, low].astype(f32) + bx1[d].astype(f32)
        ).astype(bf)
        send(part.at[2, 0, d, :, low], by2.at[d, :, low], rs.at[4, d], rr.at[4, d], near_y)
        arrived(by1.at[d], rr.at[1, d], near_y)
        part[1, 0, d, :, high] = (
            part[1, 0, d, :, high].astype(f32) + by1[d].astype(f32)
        ).astype(bf)
        send(part.at[1, 0, d, :, high], bx2.at[d, :, high], rs.at[5, d], rr.at[5, d], near_x)

    def finish(d):
        arrived(by2.at[d, :, high], rr.at[2, d], near_y)
        arrived(bx2.at[d, :, low], rr.at[3, d], near_x)
        arrived(by2.at[d, :, low], rr.at[4, d], near_y)
        arrived(bx2.at[d, :, high], rr.at[5, d], near_x)
        full = (
            part[0, 0, d].astype(f32) + bx2[d].astype(f32) + by2[d].astype(f32)
        ).astype(bf)
        if d == 0:
            back[0] = full
        else:
            done[d] = full
            send(done.at[d], back.at[d], bs.at[d], br.at[d], along(-d))

    spread(3)
    for d in order:
        third(0, d)
    spread(2)
    join(3, away[0])
    start(away[0])
    join(3, away[1])
    start(away[1])
    join(2, away[0])
    rest_y(away[0])
    for d in away[2:]:
        join(3, d)
    for d in away[1:]:
        join(2, d)
    spread(1)
    join(1, away[0])
    rest_x(away[0])
    start(away[2])
    for d in away[1:]:
        join(1, d)
    spread(0)
    pass_on(away[0])
    rest_y(away[1])
    rest_x(away[1])
    pass_on(away[1])
    start(away[3])
    rest_y(away[2])
    rest_x(away[2])
    for d in away:
        join(0, d)
    for d in range(planes):
        arrived(latents.at[1, d], kr.at[0, d], partner)
        arrived(ropes.at[1, d], kr.at[1, d], partner)
    loads["key_up"].wait()
    loads["value_up"].wait()
    starts = [
        ((plane - d + planes) % planes * 2 + (core ^ parity)) * tokens
        for parity in range(2)
        for d in range(planes)
    ]
    key_total = blocks * tokens
    key_rows = latents[...].reshape(key_total, latents.shape[-1])
    key_t = lax.dot_general(
        key_up_v[...], key_rows, (((0,), (1,)), ((), ())), preferred_element_type=f32
    )
    key_t = key_t.astype(bf).astype(f32)
    values_v[...] = jnp.dot(key_rows, value_up_v[...], preferred_element_type=f32).astype(bf)
    rope_t = jnp.concatenate(
        [ropes[parity, d].astype(f32) for parity in range(2) for d in range(planes)], axis=1
    )
    lanes = [pl.ds(pl.multiple_of(start, tokens), tokens) for start in starts]
    cos_k = jnp.concatenate([table_v[0:half, lane] for lane in lanes], axis=1)
    sin_k = jnp.concatenate([table_v[half:ROPE, lane] for lane in lanes], axis=1)
    lane_ids = lax.broadcasted_iota(jnp.int32, (1, tokens), 1)
    key_pos = jnp.concatenate([lane_ids + start for start in starts], axis=1)
    query_pos = ep * tokens + lax.broadcasted_iota(jnp.int32, (tokens, 1), 0)
    visible = key_pos <= query_pos
    rope_squares = jnp.sum(rope_t * rope_t, axis=0, keepdims=True)
    for h in range(head_count):
        nope = key_t[h * NOPE : (h + 1) * NOPE]
        squares = jnp.sum(nope * nope, axis=0, keepdims=True) + rope_squares
        factor = lax.rsqrt(squares / QKD + EPS)
        nope = nope * factor * gain_k[:NOPE]
        spun = rope_t * factor * gain_k[NOPE:]
        turned_a, turned_b = turn(spun[:half], spun[half:], cos_k, sin_k)
        turned_k[h] = jnp.concatenate([nope, turned_a, turned_b], axis=0).astype(bf)
    head_of = jnp.right_shift(
        lax.broadcasted_iota(jnp.int32, (tokens, head_count * VDIM), 1), VDIM.bit_length() - 1
    )

    def attend(h, attn):
        scores = (
            lax.dot_general(turned_q[h], turned_k[h], turned, preferred_element_type=f32)
            * QKD ** (-0.5)
        )
        scores = jnp.where(visible, scores, -1e30)
        expo = jnp.exp(scores - jnp.max(scores, axis=-1, keepdims=True))
        total = jnp.sum(expo, axis=-1, keepdims=True)
        mixed_h = jnp.dot(expo.astype(bf), values_v[...], preferred_element_type=f32) / total
        return jnp.where(head_of == h, mixed_h, attn)

    finish(away[0])
    pass_on(away[2])
    rest_y(away[3])
    rest_x(away[3])
    attn = jnp.zeros((tokens, head_count * VDIM), f32)
    for h in range(head_count // 2):
        attn = attend(h, attn)
    finish(away[1])
    pass_on(away[3])
    for h in range(head_count // 2, head_count):
        attn = attend(h, attn)
    heads[tp] = attn.astype(bf)
    for i, peer in enumerate((near_x, near_y, corner)):
        send(heads.at[tp], heads.at[tp], hs.at[i], hr.at[i], peer)
    finish(away[2])
    finish(away[3])
    for i, peer in enumerate((near_x, near_y, corner)):
        arrived(heads.at[tp ^ (i + 1)], hr.at[i], peer)
    loads["out_gain"].wait()
    loads["out_proj"].wait()
    block_f = jnp.concatenate([heads[q] for q in range(4)], axis=1).astype(f32)
    squares = jnp.mean(block_f * block_f, axis=-1, keepdims=True)
    scaled = (block_f * out_gain_v[...]).astype(bf)
    product = jnp.dot(scaled, out_proj_v[...], preferred_element_type=f32)
    mixed_ref[...] = (product * lax.rsqrt(squares + EPS)).astype(bf)

    for d in order:
        arrived(back.at[d], br.at[d], along(d))
    expert_ref[...] = jnp.dot(
        select_t[...], back[...].reshape(planes * cap, width), preferred_element_type=f32
    ).astype(bf)
    for copy in sent:
        copy.wait_send()


def fused(
    queries,
    kv_latent,
    rope_key,
    latent_gain,
    key_up,
    value_up,
    query_gain,
    key_gain,
    out_gain,
    out_proj,
    moe_input,
    moe_gain,
    expert_ids,
    route_weights,
    w_gate,
    w_up,
    w_down,
):
    f32, bf, i32 = jnp.float32, jnp.bfloat16, jnp.int32
    planes = lax.axis_size("ep") // 2
    tokens, model = moe_input.shape
    width = model // lax.axis_size("tp")
    experts, _, hidden = w_gate.shape
    cap = group_cap()
    blocks = 2 * planes
    row_total, slots = blocks * cap, blocks * CAP
    slot_total = experts * slots
    rank = kv_latent.shape[1]
    head_count = key_up.shape[1] // NOPE
    total = tokens * lax.axis_size("ep")
    v_cols = value_up.shape[1]
    table = jnp.asarray(rope_table(total))
    dma = pltpu.SemaphoreType.DMA
    vmem = pltpu.VMEM
    operands = (
        queries,
        kv_latent,
        rope_key.T,
        latent_gain.reshape(1, -1),
        key_up,
        value_up,
        query_gain.reshape(1, -1),
        key_gain.reshape(1, -1),
        out_gain.reshape(1, -1),
        out_proj,
        moe_input,
        moe_gain.reshape(1, -1),
        expert_ids.T,
        route_weights.T,
        w_gate,
        w_up,
        w_down,
        table,
    )
    mixed, expert_out = pl.pallas_call(
        functools.partial(layer_kernel, planes),
        out_shape=(
            pltpu.VMEM((tokens, out_proj.shape[1]), bf),
            pltpu.VMEM((tokens, width), bf),
        ),
        in_specs=[pl.BlockSpec(memory_space=pl.ANY)] * len(operands),
        out_specs=(pl.BlockSpec(memory_space=pltpu.VMEM),) * 2,
        scratch_shapes=[
            vmem(queries.shape, bf),
            vmem(kv_latent.shape, bf),
            vmem((1, rank), f32),
            vmem(key_up.shape, bf),
            vmem(value_up.shape, bf),
            vmem((1, QKD), f32),
            vmem((1, QKD), f32),
            vmem((1, out_gain.shape[0]), f32),
            vmem(out_proj.shape, bf),
            vmem(moe_input.shape, bf),
            vmem((1, model), f32),
            vmem((2, tokens), i32),
            vmem((2, tokens), f32),
            vmem(table.shape, f32),
            vmem((9, experts, width, hidden), bf),
            vmem((2, planes, tokens, rank), bf),
            vmem((2, planes, ROPE, tokens), bf),
            vmem((planes, cap, width), bf),
            vmem((planes, 16, PAD), bf),
            vmem((4, 2, planes, cap, width), bf),
            vmem((2, planes, 16, PAD), bf),
            vmem((head_count, QKD, tokens), bf),
            vmem((head_count, QKD, total), bf),
            vmem((total, v_cols), bf),
            vmem((4, tokens, v_cols), bf),
            vmem((tokens, planes * cap), bf),
            vmem((2, row_total // 2, slot_total // 2), bf),
            vmem((2, slot_total // 2, row_total // 2), bf),
            vmem((2, slot_total // 2, 1), f32),
            vmem((2, slot_total // 2, width), bf),
            vmem((experts, slots, hidden), f32),
            vmem((experts, slots, hidden), f32),
            vmem((2, slot_total // 2, hidden), bf),
            vmem((2, slot_total // 2, width), bf),
            vmem((4, 2, planes, cap, width), bf),
            vmem((4, planes, cap, width), bf),
            vmem((planes, cap, width // 2), bf),
            vmem((planes, cap, width // 2), bf),
            vmem((planes, cap, width), bf),
            vmem((planes, cap, width), bf),
            vmem((planes, cap, width), bf),
            vmem((planes, cap, width), bf),
            dma((15,)),
            dma((4, 4)),
            dma((4, planes)),
            dma((4, planes)),
            dma((2, 4, planes)),
            dma((2, 4, planes)),
            dma((3, planes)),
            dma((3, planes)),
            dma((4, planes)),
            dma((4, planes)),
            dma((3,)),
            dma((3,)),
            dma((4, planes)),
            dma((4, planes)),
            dma((6, planes)),
            dma((6, planes)),
            dma((planes,)),
            dma((planes,)),
        ],
        compiler_params=pltpu.CompilerParams(
            collective_id=0, has_side_effects=True, vmem_limit_bytes=62 * 2**20
        ),
        name="layer",
    )(*operands)
    return flush(mixed, expert_out)


def flush_kernel(a_ref, b_ref, x_ref, y_ref, sems):
    copies = [
        pltpu.make_async_copy(a_ref, x_ref, sems.at[0]),
        pltpu.make_async_copy(b_ref, y_ref, sems.at[1]),
    ]
    for copy in copies:
        copy.start()
    for copy in copies:
        copy.wait()


def flush(first_out, second_out):
    return pl.pallas_call(
        flush_kernel,
        out_shape=(
            jax.ShapeDtypeStruct(first_out.shape, first_out.dtype),
            jax.ShapeDtypeStruct(second_out.shape, second_out.dtype),
        ),
        in_specs=[pl.BlockSpec(memory_space=pltpu.VMEM)] * 2,
        out_specs=(pl.BlockSpec(memory_space=pl.ANY),) * 2,
        scratch_shapes=[pltpu.SemaphoreType.DMA((2,))],
        name="flush",
    )(
        pltpu.with_memory_space_constraint(first_out, pltpu.VMEM),
        pltpu.with_memory_space_constraint(second_out, pltpu.VMEM),
    )


def layer(*arrays):
    gate, stream = arrays[14], arrays[10]
    tp_count, ep_count = lax.axis_size("tp"), lax.axis_size("ep")
    fits = (
        tp_count == 4
        and ep_count == 2 * tp_count
        and 2 * gate.shape[0] == GROUP
        and stream.shape[0] == PAD
        and stream.shape[1] // tp_count == 2 * gate.shape[2]
    )
    return fused(*arrays) if fits else shards(*arrays)


def solution(mesh):
    in_specs = (
        P("ep", "tp"),
        P("ep", None),
        P("ep", None),
        P(),
        P(None, "tp"),
        P(None, "tp"),
        P(),
        P(),
        P(),
        P(None, "tp"),
        P("ep", None),
        P(),
        P("ep", None),
        P("ep", None),
        P("ep", None, "tp"),
        P("ep", None, "tp"),
        P("ep", "tp", None),
    )
    out_specs = (P("ep", "tp"), P("ep", "tp"))
    return jax.shard_map(layer, mesh=mesh, in_specs=in_specs, out_specs=out_specs, check_vma=False)
```

```python
import functools

import jax
import jax.numpy as jnp
import numpy as np
from jax import lax
from jax.experimental import pallas as pl
from jax.experimental.pallas import tpu as pltpu
from jax.sharding import PartitionSpec as P

NOPE = 64
ROPE = 32
VDIM = 64
QKD = 96
CAP = 12


EPS = 1e-06
THETA = 10000.0


def rotate_half(values_in, positions):
    half_width = ROPE // 2
    inverse = THETA ** (-jnp.arange(half_width, dtype=jnp.float32) / half_width)
    angles = positions.astype(jnp.float32)[:, None] * inverse
    cosine = jnp.cos(angles)[:, None, :]
    sine = jnp.sin(angles)[:, None, :]
    first_half = values_in[..., :half_width]
    second_half = values_in[..., half_width:]
    return jnp.concatenate(
        [first_half * cosine - second_half * sine, second_half * cosine + first_half * sine],
        axis=-1,
    )


def head_norm(values_in, gain_vec):
    return (
        values_in
        * lax.rsqrt(jnp.mean(values_in * values_in, axis=-1, keepdims=True) + EPS)
        * gain_vec
    )


def make_queries(queries, query_gain, positions):
    row_count = queries.shape[0]
    head_count = queries.shape[1] // QKD
    normed = head_norm(queries.astype(jnp.float32).reshape(row_count, head_count, QKD), query_gain)
    turned = jnp.concatenate(
        [normed[..., :NOPE], rotate_half(normed[..., NOPE:], positions)], axis=-1
    )
    return turned.astype(jnp.bfloat16)


def make_keys(latent, rope_part, latent_gain, key_up, value_up, key_gain, positions):
    row_count = latent.shape[0]
    head_count = key_up.shape[1] // NOPE
    latent_f = latent.astype(jnp.float32)
    latent_n = (
        latent_f
        * lax.rsqrt(jnp.mean(latent_f * latent_f, axis=-1, keepdims=True) + EPS)
        * latent_gain
    ).astype(jnp.bfloat16)
    key_nope = jnp.dot(latent_n, key_up, preferred_element_type=jnp.float32).astype(jnp.bfloat16)
    key_nope = lax.optimization_barrier(key_nope)
    value_rows = jnp.dot(latent_n, value_up, preferred_element_type=jnp.float32).astype(
        jnp.bfloat16
    )
    shared = jnp.broadcast_to(
        rope_part.astype(jnp.float32)[:, None, :], (row_count, head_count, ROPE)
    )
    key_full = jnp.concatenate(
        [key_nope.astype(jnp.float32).reshape(row_count, head_count, NOPE), shared], axis=-1
    )
    normed = head_norm(key_full, key_gain)
    turned = jnp.concatenate(
        [normed[..., :NOPE], rotate_half(normed[..., NOPE:], positions)], axis=-1
    )
    return (turned.astype(jnp.bfloat16), value_rows.reshape(row_count, head_count, VDIM))


def shards(
    queries,
    kv_latent,
    rope_key,
    latent_gain,
    key_up,
    value_up,
    query_gain,
    key_gain,
    out_gain,
    out_proj,
    moe_input,
    moe_gain,
    expert_ids,
    route_weights,
    w_gate,
    w_up,
    w_down,
):
    tok_rows = queries.shape[0]
    head_count = key_up.shape[1] // NOPE
    query_pos = lax.axis_index("ep") * tok_rows + jnp.arange(tok_rows, dtype=jnp.int32)
    query_rot = make_queries(queries, query_gain, query_pos)
    inv_scale = QKD ** (-0.5)
    blocks_in = (
        lax.all_gather(kv_latent, "ep", axis=0, tiled=True),
        lax.all_gather(rope_key, "ep", axis=0, tiled=True),
    )
    key_pos = jnp.arange(blocks_in[0].shape[0], dtype=jnp.int32)
    key_rot, value_rows = make_keys(
        blocks_in[0], blocks_in[1], latent_gain, key_up, value_up, key_gain, key_pos
    )
    top_prev = jnp.full((head_count, tok_rows), -1e30, jnp.float32)
    key_pos = jnp.arange(key_rot.shape[0], dtype=jnp.int32)
    scores = (
        jnp.einsum("qhd,khd->hqk", query_rot, key_rot, preferred_element_type=jnp.float32)
        * inv_scale
    )
    visible = key_pos[None, :] <= query_pos[:, None]
    scores = jnp.where(visible[None], scores, -1e30)
    top_new = jnp.maximum(top_prev, jnp.max(scores, axis=-1))
    expo = jnp.exp(scores - top_new[..., None])
    total_new = jnp.sum(expo, axis=-1)
    accum_new = jnp.einsum(
        "hqk,khd->hqd", expo.astype(jnp.bfloat16), value_rows, preferred_element_type=jnp.float32
    )
    attn = (accum_new / total_new[..., None]).astype(jnp.bfloat16)
    attn = attn.transpose(1, 0, 2).reshape(tok_rows, head_count * VDIM)
    block_f = lax.all_gather(attn, "tp", axis=1, tiled=True).astype(jnp.float32)
    scaled = (block_f * out_gain[None, :]).astype(jnp.bfloat16)
    product = jnp.dot(scaled, out_proj, preferred_element_type=jnp.float32)
    product, squares = (product, jnp.sum(block_f * block_f, axis=-1))
    mixed = (product * lax.rsqrt(squares / out_gain.shape[0] + EPS)[:, None]).astype(jnp.bfloat16)
    row_count = moe_input.shape[0]
    top_count = expert_ids.shape[1]
    local_experts = w_gate.shape[0]
    ep_count = lax.axis_size("ep")
    expert_count = local_experts * ep_count
    stream_f = moe_input.astype(jnp.float32)
    normed = (
        stream_f * lax.rsqrt(jnp.mean(stream_f * stream_f, axis=-1, keepdims=True) + EPS) * moe_gain
    ).astype(jnp.bfloat16)
    flat_ids = expert_ids.reshape(-1)
    onehot = (flat_ids[:, None] == jnp.arange(expert_count, dtype=jnp.int32)[None, :]).astype(
        jnp.int32
    )
    slot_rank = jnp.sum((jnp.cumsum(onehot, axis=0) - onehot) * onehot, axis=1)
    slot_index = flat_ids * CAP + slot_rank
    token_index = jnp.arange(row_count * top_count, dtype=jnp.int32) // top_count
    slot_token = jnp.zeros((expert_count * CAP,), jnp.int32).at[slot_index].set(token_index)
    slot_used = jnp.zeros((expert_count * CAP,), jnp.bool_).at[slot_index].set(True)
    outgoing = jnp.where(slot_used[:, None], normed[slot_token], jnp.zeros((), jnp.bfloat16))
    outgoing = outgoing.reshape(ep_count, local_experts, CAP, normed.shape[1])
    piece_width = normed.shape[1] // lax.axis_size("tp")
    my_columns = lax.dynamic_slice_in_dim(
        outgoing, lax.axis_index("tp") * piece_width, piece_width, 3
    )
    arrived_part = lax.all_to_all(my_columns, "ep", split_axis=0, concat_axis=0, tiled=True)
    piece = lax.all_gather(arrived_part, "tp", axis=3, tiled=True)
    gate_acc = jnp.einsum("secd,edf->secf", piece, w_gate, preferred_element_type=jnp.float32)
    upper_acc = jnp.einsum("secd,edf->secf", piece, w_up, preferred_element_type=jnp.float32)
    hidden = (jax.nn.silu(gate_acc) * upper_acc).astype(jnp.bfloat16)
    out_cols = w_down.shape[2] // lax.axis_size("tp")
    term = jnp.einsum("secf,efd->dsec", hidden, w_down, preferred_element_type=jnp.float32)
    summed = lax.psum_scatter(
        term.reshape(lax.axis_size("tp") * out_cols, -1).astype(jnp.bfloat16),
        "tp",
        scatter_dimension=0,
        tiled=True,
    )
    expert_y = summed.T.reshape(ep_count, local_experts * CAP, out_cols)
    returned_rows = lax.all_to_all(expert_y, "ep", split_axis=0, concat_axis=0, tiled=True).reshape(
        expert_count * CAP, out_cols
    )
    picked = returned_rows[slot_index].reshape(row_count, top_count, out_cols).astype(jnp.float32)
    expert_out = jnp.sum(picked * route_weights[..., None], axis=1).astype(jnp.bfloat16)
    return (mixed, expert_out)


MESH = pl.DeviceIdType.MESH
GROUP = 8
PAD = 128


def group_cap():
    return GROUP * CAP // 2


def rdma(src, dst, send_sem, recv_sem, device):
    copy = pltpu.make_async_remote_copy(
        src_ref=src,
        dst_ref=dst,
        send_sem=send_sem,
        recv_sem=recv_sem,
        device_id=device,
        device_id_type=MESH,
    )
    copy.start()
    return copy


def arrived(dst, sem, device):
    pltpu.make_async_remote_copy(
        src_ref=dst,
        dst_ref=dst,
        send_sem=sem,
        recv_sem=sem,
        device_id=device,
        device_id_type=MESH,
    ).wait_recv()


def places(planes):
    ep = lax.axis_index("ep")
    tp = lax.axis_index("tp")
    plane = ep // 2
    core = ep % 2

    def along(offset):
        return (lax.rem(plane + offset + planes, planes) * 2 + core, tp)

    partner = (plane * 2 + 1 - core, tp)
    near_x = (ep, tp ^ 1)
    near_y = (ep, tp ^ 2)
    corner = (ep, tp ^ 3)
    return tp, along, partner, near_x, near_y, corner


def rope_table(total):
    half = ROPE // 2
    inverse = np.float32(THETA) ** (-np.arange(half, dtype=np.float32) / np.float32(half))
    angles = np.arange(total, dtype=np.float32)[None, :] * inverse[:, None]
    return np.concatenate([np.cos(angles), np.sin(angles)], axis=0).astype(np.float32)


def turn(first_half, second_half, cosine, sine):
    return (
        first_half * cosine - second_half * sine,
        second_half * cosine + first_half * sine,
    )


def to_column(row):
    size = row.shape[1]
    rows = lax.broadcasted_iota(jnp.int32, (size, size), 0)
    cols = lax.broadcasted_iota(jnp.int32, (size, size), 1)
    return jnp.sum(jnp.where(rows == cols, row, 0.0), axis=1, keepdims=True)


def layer_kernel(
    planes,
    queries_in,
    latent_in,
    rope_in,
    latent_gain_in,
    key_up_in,
    value_up_in,
    query_gain_in,
    key_gain_in,
    out_gain_in,
    out_proj_in,
    stream_in,
    moe_gain_in,
    ids_in,
    weights_in,
    gate_ref,
    up_ref,
    down_ref,
    table_in,
    mixed_ref,
    expert_ref,
    queries_v,
    latent_v,
    latent_gain_v,
    key_up_v,
    value_up_v,
    query_gain_v,
    key_gain_v,
    out_gain_v,
    out_proj_v,
    stream_v,
    moe_gain_v,
    ids_v,
    weights_v,
    table_v,
    wbuf,
    latents,
    ropes,
    outgoing,
    metas_out,
    rows_ref,
    metas,
    turned_q,
    turned_k,
    values_v,
    heads,
    select_t,
    place_v,
    place_t,
    slot_w,
    taken,
    gate_acc,
    up_acc,
    hidden_v,
    given,
    part,
    other,
    bx1,
    by1,
    bx2,
    by2,
    done,
    back,
    loc,
    ws,
    zs,
    zr,
    xs,
    xr,
    ks,
    kr,
    ps,
    pr,
    hs,
    hr,
    cs,
    cr,
    rs,
    rr,
    bs,
    br,
):
    f32, bf = jnp.float32, jnp.bfloat16
    ep = lax.axis_index("ep")
    plane, core = ep // 2, ep % 2
    tp, along, partner, near_x, near_y, corner = places(planes)
    peers = [along(d) for d in range(1, planes)] + [partner, near_x, near_y, corner]
    barrier = pltpu.get_barrier_semaphore()
    for peer in peers:
        pl.semaphore_signal(barrier, inc=1, device_id=peer, device_id_type=MESH)

    blocks = 2 * planes
    tokens, model = stream_in.shape
    cap, width = outgoing.shape[1], outgoing.shape[2]
    experts, hidden = gate_ref.shape[0], gate_ref.shape[2]
    row_total, slots = blocks * cap, blocks * CAP
    slot_total = experts * slots
    quarter_rows = tokens // 4
    half_r, half_w = quarter_rows // 2, width // 2
    low, high = pl.ds(0, half_w), pl.ds(half_w, half_w)
    halves = (low, high)
    head_count = key_up_in.shape[1] // NOPE
    order = sorted(range(1, planes), key=lambda d: (min(d, planes - d), d))
    away = sorted(range(1, planes), key=lambda d: (-min(d, planes - d), d)) + [0]
    turned = (((0,), (0,)), ((), ()))
    across = (((1,), (1,)), ((), ()))

    loads = {}

    def load(name, source, target):
        copy = pltpu.make_async_copy(source, target, loc.at[len(loads)])
        copy.start()
        loads[name] = copy

    load("ids", ids_in, ids_v)
    load("weights", weights_in, weights_v)
    load("stream", stream_in, stream_v)
    load("moe_gain", moe_gain_in, moe_gain_v)
    load("latent", latent_in, latent_v)
    load("latent_gain", latent_gain_in, latent_gain_v)
    load("rope", rope_in, ropes.at[0, 0])
    load("queries", queries_in, queries_v)
    load("query_gain", query_gain_in, query_gain_v)
    load("key_gain", key_gain_in, key_gain_v)
    load("table", table_in, table_v)
    load("key_up", key_up_in, key_up_v)
    load("value_up", value_up_in, value_up_v)

    sent = []

    def send(src, dst, send_sem, recv_sem, device):
        sent.append(rdma(src, dst, send_sem, recv_sem, device))

    def quarter(which):
        return pl.ds(pl.multiple_of(which * quarter_rows, quarter_rows), quarter_rows)

    loads["ids"].wait()
    loads["weights"].wait()
    ids = ids_v[...]
    local_ids = ids & (GROUP - 1)
    group = jnp.right_shift(ids[0:1], GROUP.bit_length() - 1)
    offset = jnp.where(group >= plane, group - plane, group - plane + planes)
    in_group = lax.broadcasted_iota(jnp.int32, (8, tokens), 0) == offset
    names = lax.broadcasted_iota(jnp.int32, (planes * GROUP, tokens), 0)
    hit = [names == offset * GROUP + local_ids[k : k + 1] for k in range(2)]
    counted = jnp.concatenate(
        [in_group.astype(f32), hit[0].astype(f32) + hit[1].astype(f32)], axis=0
    ).astype(bf)
    before = (
        lax.broadcasted_iota(jnp.int32, (tokens, tokens), 0)
        < lax.broadcasted_iota(jnp.int32, (tokens, tokens), 1)
    ).astype(f32).astype(bf)
    earlier = jnp.dot(counted, before, preferred_element_type=f32)
    rank = jnp.sum(jnp.where(in_group, earlier[0:8], 0.0), axis=0, keepdims=True).astype(jnp.int32)
    codes = [
        local_ids[k : k + 1].astype(f32) * CAP
        + jnp.sum(jnp.where(hit[k], earlier[8:], 0.0), axis=0, keepdims=True)
        + 1.0
        for k in range(2)
    ]
    route = weights_v[...]
    route_high = route.astype(bf).astype(f32)
    route_low = route - route_high
    line = lax.broadcasted_iota(jnp.int32, (16, tokens), 0)
    meta = jnp.zeros((16, tokens), f32)
    meta_rows = codes + [route_high[0:1], route_high[1:2], route_low[0:1], route_low[1:2]]
    for i, row in enumerate(meta_rows):
        meta = jnp.where(line == i, row, meta)
    select = (
        lax.broadcasted_iota(jnp.int32, (planes * cap, tokens), 0) == offset * cap + rank
    ).astype(f32)
    select_b = select.astype(bf)
    wide = (
        lax.broadcasted_iota(jnp.int32, (planes * PAD, tokens), 0) == offset * PAD + rank
    ).astype(f32).astype(bf)
    meta_all = lax.dot_general(meta.astype(bf), wide, across, preferred_element_type=f32).astype(bf)
    for d in range(planes):
        metas_out[d] = meta_all[:, d * PAD : (d + 1) * PAD]
    metas[0, 0] = meta_all[:, 0:PAD]

    loads["stream"].wait()
    loads["moe_gain"].wait()
    gate_in, up_in, down_in = [], [], {}
    for s in range(4):
        depth = pl.ds(pl.multiple_of((tp ^ s) * width, width), width)
        gate_in.append(
            pltpu.make_async_copy(gate_ref.at[:, depth, :], wbuf.at[s], ws.at[0, s])
        )
        up_in.append(pltpu.make_async_copy(up_ref.at[:, depth, :], wbuf.at[4 + s], ws.at[1, s]))
        gate_in[s].start()
        up_in[s].start()
    down_slot = (1, 4, 0, 8)
    pieces = width // hidden

    def fetch_down(s):
        for piece in range(pieces):
            start = pl.multiple_of((tp ^ s) * width + piece * hidden, hidden)
            copy = pltpu.make_async_copy(
                down_ref.at[:, :, pl.ds(start, hidden)],
                wbuf.at[down_slot[s], :, pl.ds(piece * hidden, hidden), :],
                ws.at[2 + piece, s],
            )
            copy.start()
            down_in[s, piece] = copy

    fetch_down(3)
    load("out_gain", out_gain_in, out_gain_v)
    load("out_proj", out_proj_in, out_proj_v)

    stream_f = stream_v[...].astype(f32)
    scale = lax.rsqrt(jnp.mean(stream_f * stream_f, axis=-1, keepdims=True) + EPS)
    own_cols = pl.ds(pl.multiple_of(tp * width, width), width)
    own_normed = (
        stream_v[:, own_cols].astype(f32) * scale * moe_gain_v[:, own_cols]
    ).astype(bf)
    out_rows = jnp.dot(select_b[cap:], own_normed, preferred_element_type=f32).astype(bf)
    for d in order:
        outgoing[d] = out_rows[(d - 1) * cap : d * cap]
    pl.semaphore_wait(barrier, len(peers))
    for d in order:
        send(metas_out.at[d], metas.at[0, d], zs.at[2, d], zr.at[2, d], along(d))
    for d in order:
        send(outgoing.at[d], rows_ref.at[tp, 0, d], zs.at[3, d], zr.at[3, d], along(d))
    for q in range(4):
        cols = slice(q * width, (q + 1) * width)
        normed_q = (stream_v[:, cols].astype(f32) * scale * moe_gain_v[:, cols]).astype(bf)
        rows_ref[q, 0, 0] = jnp.dot(select_b[0:cap], normed_q, preferred_element_type=f32).astype(bf)
    send(rows_ref.at[:, 0, 0], rows_ref.at[:, 1, 0], ps.at[0, 0], pr.at[0, 0], partner)
    send(metas_out.at[0], metas.at[1, 0], ks.at[2, 0], kr.at[2, 0], partner)
    loads["latent"].wait()
    loads["latent_gain"].wait()
    latent_f = latent_v[...].astype(f32)
    latents[0, 0] = (
        latent_f
        * lax.rsqrt(jnp.mean(latent_f * latent_f, axis=-1, keepdims=True) + EPS)
        * latent_gain_v[...]
    ).astype(bf)
    loads["rope"].wait()
    select_t[...] = jnp.transpose(select).astype(bf)

    def first(kind, d):
        if kind == 0:
            mine = latents.at[0, d, quarter(tp)]
            arrived(mine, zr.at[0, d], along(-d))
        else:
            mine = rows_ref.at[tp, 0, d]
            arrived(mine, zr.at[3, d], along(-d))
        send(mine, mine, xs.at[kind, 0, d], xr.at[kind, 0, d], near_x)
        send(mine, mine, xs.at[kind, 1, d], xr.at[kind, 1, d], near_y)
        if kind == 0:
            arrived(ropes.at[0, d], zr.at[1, d], along(-d))
            send(ropes.at[0, d], ropes.at[1, d], ks.at[1, d], kr.at[1, d], partner)
        else:
            send(mine, rows_ref.at[tp, 1, d], ps.at[0, d], pr.at[0, d], partner)

    def half_of(kind, flip, d, side):
        if kind == 0:
            start = (tp ^ flip) * quarter_rows + side * half_r
            return latents.at[0, d, pl.ds(pl.multiple_of(start, half_r), half_r)]
        return rows_ref.at[tp ^ flip, 0, d, :, halves[side]]

    def whole_of(kind, flip, d):
        if kind == 0:
            return latents.at[0, d, quarter(tp ^ flip)]
        return rows_ref.at[tp ^ flip, 0, d]

    def second(kind, d):
        arrived(whole_of(kind, 1, d), xr.at[kind, 0, d], near_x)
        piece = half_of(kind, 1, d, 0)
        send(piece, piece, xs.at[kind, 2, d], xr.at[kind, 2, d], near_y)
        arrived(whole_of(kind, 2, d), xr.at[kind, 1, d], near_y)
        piece = half_of(kind, 2, d, 1)
        send(piece, piece, xs.at[kind, 3, d], xr.at[kind, 3, d], near_x)
        if kind == 1:
            for flip in (1, 2):
                send(
                    rows_ref.at[tp ^ flip, 0, d],
                    rows_ref.at[tp ^ flip, 1, d],
                    ps.at[flip, d],
                    pr.at[flip, d],
                    partner,
                )

    def third(kind, d):
        arrived(half_of(kind, 3, d, 0), xr.at[kind, 2, d], near_y)
        arrived(half_of(kind, 3, d, 1), xr.at[kind, 3, d], near_x)
        if kind == 0:
            send(latents.at[0, d], latents.at[1, d], ks.at[0, d], kr.at[0, d], partner)
        else:
            mine = rows_ref.at[tp ^ 3, 0, d]
            send(mine, rows_ref.at[tp ^ 3, 1, d], ps.at[3, d], pr.at[3, d], partner)

    loads["queries"].wait()
    loads["query_gain"].wait()
    loads["key_gain"].wait()
    loads["table"].wait()
    half = ROPE // 2
    query_t = jnp.transpose(queries_v[...].astype(f32))
    gain_q = to_column(query_gain_v[...])
    gain_k = to_column(key_gain_v[...])
    own_lanes = pl.ds(pl.multiple_of(ep * tokens, tokens), tokens)
    cos_q, sin_q = table_v[0:half, own_lanes], table_v[half:ROPE, own_lanes]
    for h in range(head_count):
        z = query_t[h * QKD : (h + 1) * QKD]
        z = z * lax.rsqrt(jnp.mean(z * z, axis=0, keepdims=True) + EPS) * gain_q
        turned_a, turned_b = turn(z[NOPE : NOPE + half], z[NOPE + half :], cos_q, sin_q)
        turned_q[h] = jnp.concatenate([z[:NOPE], turned_a, turned_b], axis=0).astype(bf)

    each = planes * CAP

    def both(ref, e):
        mine = slice(e * each, (e + 1) * each)
        return jnp.concatenate([ref[0, mine, :], ref[1, mine, :]], axis=0)

    def feed(s):
        for d in range(planes):
            if s == 0 and d == 0:
                arrived(rows_ref.at[:, 1, 0], pr.at[0, 0], partner)
            elif d > 0:
                arrived(rows_ref.at[tp ^ s, 1, d], pr.at[s, d], partner)
        for parity in range(2):
            rows = rows_ref[tp ^ s, parity].reshape(planes * cap, width)
            taken[parity] = jnp.dot(
                place_t[parity], rows, preferred_element_type=f32
            ).astype(bf)
        gate_in[s].wait()
        up_in[s].wait()
        for e in range(experts):
            picked = both(taken, e)
            gate = jnp.dot(picked, wbuf[s, e], preferred_element_type=f32)
            upper = jnp.dot(picked, wbuf[4 + s, e], preferred_element_type=f32)
            if s > 0:
                gate += gate_acc[e]
                upper += up_acc[e]
            if s < 3:
                gate_acc[e] = gate
                up_acc[e] = upper
            else:
                act = (gate / (1.0 + jnp.exp(-gate)) * upper * both(slot_w, e)).astype(bf)
                for parity in range(2):
                    hidden_v[parity, e * each : (e + 1) * each] = act[
                        parity * each : (parity + 1) * each
                    ]

    for d in order:
        arrived(metas.at[0, d], zr.at[2, d], along(-d))
        send(metas.at[0, d], metas.at[1, d], ks.at[2, d], kr.at[2, d], partner)
    spot = (
        lax.broadcasted_iota(jnp.int32, (cap, PAD), 0)
        == lax.broadcasted_iota(jnp.int32, (cap, PAD), 1)
    ).astype(f32).astype(bf)
    side_rows, side_slots = planes * cap, experts * planes * CAP
    plane_of = jnp.concatenate(
        [jnp.full((cap, 1), d, jnp.int32) for d in range(planes)], axis=0
    )
    slot_ids = lax.broadcasted_iota(jnp.int32, (side_rows, side_slots), 1)
    def settle(parity):
        info = jnp.concatenate(
            [
                lax.dot_general(spot, metas[parity, d], across, preferred_element_type=f32)
                for d in range(planes)
            ],
            axis=0,
        )
        info_b = info.astype(bf)
        place = jnp.zeros((side_rows, side_slots), f32)
        placed_t = jnp.zeros((side_slots, side_rows), f32)
        slot_weights = jnp.zeros((side_slots, 1), f32)
        for k in range(2):
            column = info[:, k : k + 1]
            code = column.astype(jnp.int32) - 1 - core * (experts * CAP)
            inside = (column > 0.5) & (code >= 0) & (code < experts * CAP)
            expert = jnp.zeros_like(code)
            for e in range(1, experts):
                expert += (code >= e * CAP).astype(jnp.int32)
            where = expert * ((planes - 1) * CAP) + plane_of * CAP + code
            match = (slot_ids == jnp.where(inside, where, -1)).astype(f32)
            match_t = jnp.transpose(match)
            place += match
            placed_t += match_t
            found = jnp.dot(match_t.astype(bf), info_b, preferred_element_type=f32)
            slot_weights += found[:, 2 + k : 3 + k] + found[:, 4 + k : 5 + k]
        place_v[parity] = place.astype(bf)
        place_t[parity] = placed_t.astype(bf)
        slot_w[parity] = slot_weights

    settle(0)
    first(1, order[0])
    for d in range(planes):
        arrived(metas.at[1, d], kr.at[2, d], partner)
    settle(1)
    first(1, order[1])
    second(1, order[0])
    first(1, order[2])
    own_part = latents.at[0, 0, quarter(tp)]
    for d in order:
        send(own_part, latents.at[0, d, quarter(tp)], zs.at[0, d], zr.at[0, d], along(d))
        send(ropes.at[0, 0], ropes.at[0, d], zs.at[1, d], zr.at[1, d], along(d))
    send(latents.at[0, 0], latents.at[1, 0], ks.at[0, 0], kr.at[0, 0], partner)
    send(ropes.at[0, 0], ropes.at[1, 0], ks.at[1, 0], kr.at[1, 0], partner)

    second(1, order[1])
    feed(0)
    fetch_down(2)
    fetch_down(1)
    second(1, order[-1])
    for d in order[:-1]:
        third(1, d)
    for d in order:
        first(0, d)
    feed(1)
    fetch_down(0)
    third(1, order[-1])
    for d in order[:-1]:
        second(0, d)
    feed(2)
    second(0, order[-1])
    feed(3)
    def spread(s):
        for piece in range(pieces):
            down_in[s, piece].wait()
        for e in range(experts):
            act = both(hidden_v, e)
            for piece in range(pieces):
                cols = slice(piece * hidden, (piece + 1) * hidden)
                result = jnp.dot(
                    act, wbuf[down_slot[s], e, cols, :], preferred_element_type=f32
                ).astype(bf)
                for parity in range(2):
                    given[parity, e * each : (e + 1) * each, cols] = result[
                        parity * each : (parity + 1) * each
                    ]
        for parity in (1, 0):
            summed = jnp.dot(place_v[parity], given[parity], preferred_element_type=f32).astype(bf)
            part[s, parity] = summed.reshape(planes, cap, width)
        for d in away:
            send(part.at[s, 1, d], other.at[s, d], cs.at[s, d], cr.at[s, d], partner)

    def join(s, d):
        arrived(other.at[s, d], cr.at[s, d], partner)
        part[s, 0, d] = (part[s, 0, d].astype(f32) + other[s, d].astype(f32)).astype(bf)

    def start(d):
        send(part.at[3, 0, d, :, low], bx1.at[d], rs.at[0, d], rr.at[0, d], near_x)
        send(part.at[3, 0, d, :, high], by1.at[d], rs.at[1, d], rr.at[1, d], near_y)

    def rest_y(d):
        send(part.at[2, 0, d, :, high], by2.at[d, :, high], rs.at[2, d], rr.at[2, d], near_y)

    def rest_x(d):
        send(part.at[1, 0, d, :, low], bx2.at[d, :, low], rs.at[3, d], rr.at[3, d], near_x)

    def pass_on(d):
        arrived(bx1.at[d], rr.at[0, d], near_x)
        part[2, 0, d, :, low] = (
            part[2, 0, d, :, low].astype(f32) + bx1[d].astype(f32)
        ).astype(bf)
        send(part.at[2, 0, d, :, low], by2.at[d, :, low], rs.at[4, d], rr.at[4, d], near_y)
        arrived(by1.at[d], rr.at[1, d], near_y)
        part[1, 0, d, :, high] = (
            part[1, 0, d, :, high].astype(f32) + by1[d].astype(f32)
        ).astype(bf)
        send(part.at[1, 0, d, :, high], bx2.at[d, :, high], rs.at[5, d], rr.at[5, d], near_x)

    def finish(d):
        arrived(by2.at[d, :, high], rr.at[2, d], near_y)
        arrived(bx2.at[d, :, low], rr.at[3, d], near_x)
        arrived(by2.at[d, :, low], rr.at[4, d], near_y)
        arrived(bx2.at[d, :, high], rr.at[5, d], near_x)
        full = (
            part[0, 0, d].astype(f32) + bx2[d].astype(f32) + by2[d].astype(f32)
        ).astype(bf)
        if d == 0:
            back[0] = full
        else:
            done[d] = full
            send(done.at[d], back.at[d], bs.at[d], br.at[d], along(-d))

    spread(3)
    spread(2)
    spread(1)
    join(3, away[0])
    start(away[0])
    join(3, away[1])
    start(away[1])
    join(2, away[0])
    rest_y(away[0])
    for d in away[2:]:
        join(3, d)
    for d in away[1:]:
        join(2, d)
    for d in order:
        third(0, d)
    join(1, away[0])
    rest_x(away[0])
    start(away[2])
    for d in away[1:]:
        join(1, d)
    spread(0)
    pass_on(away[0])
    rest_y(away[1])
    rest_x(away[1])
    pass_on(away[1])
    start(away[3])
    rest_y(away[2])
    rest_x(away[2])
    for d in away:
        join(0, d)
    for d in range(planes):
        arrived(latents.at[1, d], kr.at[0, d], partner)
        arrived(ropes.at[1, d], kr.at[1, d], partner)
    loads["key_up"].wait()
    loads["value_up"].wait()
    starts = [
        ((plane - d + planes) % planes * 2 + (core ^ parity)) * tokens
        for parity in range(2)
        for d in range(planes)
    ]
    key_total = blocks * tokens
    key_rows = latents[...].reshape(key_total, latents.shape[-1])
    key_t = lax.dot_general(
        key_up_v[...], key_rows, (((0,), (1,)), ((), ())), preferred_element_type=f32
    )
    key_t = key_t.astype(bf).astype(f32)
    values_v[...] = jnp.dot(key_rows, value_up_v[...], preferred_element_type=f32).astype(bf)
    rope_t = jnp.concatenate(
        [ropes[parity, d].astype(f32) for parity in range(2) for d in range(planes)], axis=1
    )
    lanes = [pl.ds(pl.multiple_of(start, tokens), tokens) for start in starts]
    cos_k = jnp.concatenate([table_v[0:half, lane] for lane in lanes], axis=1)
    sin_k = jnp.concatenate([table_v[half:ROPE, lane] for lane in lanes], axis=1)
    lane_ids = lax.broadcasted_iota(jnp.int32, (1, tokens), 1)
    key_pos = jnp.concatenate([lane_ids + start for start in starts], axis=1)
    query_pos = ep * tokens + lax.broadcasted_iota(jnp.int32, (tokens, 1), 0)
    visible = key_pos <= query_pos
    rope_squares = jnp.sum(rope_t * rope_t, axis=0, keepdims=True)
    for h in range(head_count):
        nope = key_t[h * NOPE : (h + 1) * NOPE]
        squares = jnp.sum(nope * nope, axis=0, keepdims=True) + rope_squares
        factor = lax.rsqrt(squares / QKD + EPS)
        nope = nope * factor * gain_k[:NOPE]
        spun = rope_t * factor * gain_k[NOPE:]
        turned_a, turned_b = turn(spun[:half], spun[half:], cos_k, sin_k)
        turned_k[h] = jnp.concatenate([nope, turned_a, turned_b], axis=0).astype(bf)
    head_of = jnp.right_shift(
        lax.broadcasted_iota(jnp.int32, (tokens, head_count * VDIM), 1), VDIM.bit_length() - 1
    )

    def attend(h, attn):
        scores = (
            lax.dot_general(turned_q[h], turned_k[h], turned, preferred_element_type=f32)
            * QKD ** (-0.5)
        )
        scores = jnp.where(visible, scores, -1e30)
        expo = jnp.exp(scores - jnp.max(scores, axis=-1, keepdims=True))
        total = jnp.sum(expo, axis=-1, keepdims=True)
        mixed_h = jnp.dot(expo.astype(bf), values_v[...], preferred_element_type=f32) / total
        return jnp.where(head_of == h, mixed_h, attn)

    finish(away[0])
    pass_on(away[2])
    rest_y(away[3])
    rest_x(away[3])
    attn = jnp.zeros((tokens, head_count * VDIM), f32)
    for h in range(head_count // 2):
        attn = attend(h, attn)
    finish(away[1])
    pass_on(away[3])
    for h in range(head_count // 2, head_count):
        attn = attend(h, attn)
    heads[tp] = attn.astype(bf)
    for i, peer in enumerate((near_x, near_y, corner)):
        send(heads.at[tp], heads.at[tp], hs.at[i], hr.at[i], peer)
    finish(away[2])
    finish(away[3])
    for i, peer in enumerate((near_x, near_y, corner)):
        arrived(heads.at[tp ^ (i + 1)], hr.at[i], peer)
    loads["out_gain"].wait()
    loads["out_proj"].wait()
    block_f = jnp.concatenate([heads[q] for q in range(4)], axis=1).astype(f32)
    squares = jnp.mean(block_f * block_f, axis=-1, keepdims=True)
    scaled = (block_f * out_gain_v[...]).astype(bf)
    product = jnp.dot(scaled, out_proj_v[...], preferred_element_type=f32)
    mixed_ref[...] = (product * lax.rsqrt(squares + EPS)).astype(bf)

    for d in order:
        arrived(back.at[d], br.at[d], along(d))
    expert_ref[...] = jnp.dot(
        select_t[...], back[...].reshape(planes * cap, width), preferred_element_type=f32
    ).astype(bf)
    for copy in sent:
        copy.wait_send()


def fused(
    queries,
    kv_latent,
    rope_key,
    latent_gain,
    key_up,
    value_up,
    query_gain,
    key_gain,
    out_gain,
    out_proj,
    moe_input,
    moe_gain,
    expert_ids,
    route_weights,
    w_gate,
    w_up,
    w_down,
):
    f32, bf, i32 = jnp.float32, jnp.bfloat16, jnp.int32
    planes = lax.axis_size("ep") // 2
    tokens, model = moe_input.shape
    width = model // lax.axis_size("tp")
    experts, _, hidden = w_gate.shape
    cap = group_cap()
    blocks = 2 * planes
    row_total, slots = blocks * cap, blocks * CAP
    slot_total = experts * slots
    rank = kv_latent.shape[1]
    head_count = key_up.shape[1] // NOPE
    total = tokens * lax.axis_size("ep")
    v_cols = value_up.shape[1]
    table = jnp.asarray(rope_table(total))
    dma = pltpu.SemaphoreType.DMA
    vmem = pltpu.VMEM
    operands = (
        queries,
        kv_latent,
        rope_key.T,
        latent_gain.reshape(1, -1),
        key_up,
        value_up,
        query_gain.reshape(1, -1),
        key_gain.reshape(1, -1),
        out_gain.reshape(1, -1),
        out_proj,
        moe_input,
        moe_gain.reshape(1, -1),
        expert_ids.T,
        route_weights.T,
        w_gate,
        w_up,
        w_down,
        table,
    )
    mixed, expert_out = pl.pallas_call(
        functools.partial(layer_kernel, planes),
        out_shape=(
            pltpu.VMEM((tokens, out_proj.shape[1]), bf),
            pltpu.VMEM((tokens, width), bf),
        ),
        in_specs=[pl.BlockSpec(memory_space=pl.ANY)] * len(operands),
        out_specs=(pl.BlockSpec(memory_space=pltpu.VMEM),) * 2,
        scratch_shapes=[
            vmem(queries.shape, bf),
            vmem(kv_latent.shape, bf),
            vmem((1, rank), f32),
            vmem(key_up.shape, bf),
            vmem(value_up.shape, bf),
            vmem((1, QKD), f32),
            vmem((1, QKD), f32),
            vmem((1, out_gain.shape[0]), f32),
            vmem(out_proj.shape, bf),
            vmem(moe_input.shape, bf),
            vmem((1, model), f32),
            vmem((2, tokens), i32),
            vmem((2, tokens), f32),
            vmem(table.shape, f32),
            vmem((9, experts, width, hidden), bf),
            vmem((2, planes, tokens, rank), bf),
            vmem((2, planes, ROPE, tokens), bf),
            vmem((planes, cap, width), bf),
            vmem((planes, 16, PAD), bf),
            vmem((4, 2, planes, cap, width), bf),
            vmem((2, planes, 16, PAD), bf),
            vmem((head_count, QKD, tokens), bf),
            vmem((head_count, QKD, total), bf),
            vmem((total, v_cols), bf),
            vmem((4, tokens, v_cols), bf),
            vmem((tokens, planes * cap), bf),
            vmem((2, row_total // 2, slot_total // 2), bf),
            vmem((2, slot_total // 2, row_total // 2), bf),
            vmem((2, slot_total // 2, 1), f32),
            vmem((2, slot_total // 2, width), bf),
            vmem((experts, slots, hidden), f32),
            vmem((experts, slots, hidden), f32),
            vmem((2, slot_total // 2, hidden), bf),
            vmem((2, slot_total // 2, width), bf),
            vmem((4, 2, planes, cap, width), bf),
            vmem((4, planes, cap, width), bf),
            vmem((planes, cap, width // 2), bf),
            vmem((planes, cap, width // 2), bf),
            vmem((planes, cap, width), bf),
            vmem((planes, cap, width), bf),
            vmem((planes, cap, width), bf),
            vmem((planes, cap, width), bf),
            dma((15,)),
            dma((4, 4)),
            dma((4, planes)),
            dma((4, planes)),
            dma((2, 4, planes)),
            dma((2, 4, planes)),
            dma((3, planes)),
            dma((3, planes)),
            dma((4, planes)),
            dma((4, planes)),
            dma((3,)),
            dma((3,)),
            dma((4, planes)),
            dma((4, planes)),
            dma((6, planes)),
            dma((6, planes)),
            dma((planes,)),
            dma((planes,)),
        ],
        compiler_params=pltpu.CompilerParams(
            collective_id=0, has_side_effects=True, vmem_limit_bytes=62 * 2**20
        ),
        name="layer",
    )(*operands)
    return flush(mixed, expert_out)


def flush_kernel(a_ref, b_ref, x_ref, y_ref, sems):
    copies = [
        pltpu.make_async_copy(a_ref, x_ref, sems.at[0]),
        pltpu.make_async_copy(b_ref, y_ref, sems.at[1]),
    ]
    for copy in copies:
        copy.start()
    for copy in copies:
        copy.wait()


def flush(first_out, second_out):
    return pl.pallas_call(
        flush_kernel,
        out_shape=(
            jax.ShapeDtypeStruct(first_out.shape, first_out.dtype),
            jax.ShapeDtypeStruct(second_out.shape, second_out.dtype),
        ),
        in_specs=[pl.BlockSpec(memory_space=pltpu.VMEM)] * 2,
        out_specs=(pl.BlockSpec(memory_space=pl.ANY),) * 2,
        scratch_shapes=[pltpu.SemaphoreType.DMA((2,))],
        name="flush",
    )(
        pltpu.with_memory_space_constraint(first_out, pltpu.VMEM),
        pltpu.with_memory_space_constraint(second_out, pltpu.VMEM),
    )


def layer(*arrays):
    gate, stream = arrays[14], arrays[10]
    tp_count, ep_count = lax.axis_size("tp"), lax.axis_size("ep")
    fits = (
        tp_count == 4
        and ep_count == 2 * tp_count
        and 2 * gate.shape[0] == GROUP
        and stream.shape[0] == PAD
        and stream.shape[1] // tp_count == 2 * gate.shape[2]
    )
    return fused(*arrays) if fits else shards(*arrays)


def solution(mesh):
    in_specs = (
        P("ep", "tp"),
        P("ep", None),
        P("ep", None),
        P(),
        P(None, "tp"),
        P(None, "tp"),
        P(),
        P(),
        P(),
        P(None, "tp"),
        P("ep", None),
        P(),
        P("ep", None),
        P("ep", None),
        P("ep", None, "tp"),
        P("ep", None, "tp"),
        P("ep", "tp", None),
    )
    out_specs = (P("ep", "tp"), P("ep", "tp"))
    return jax.shard_map(layer, mesh=mesh, in_specs=in_specs, out_specs=out_specs, check_vma=False)
```
